512 devices in a mesh: ep: 128 (over z, x, core), tp: 4 (over y).
Axes of the slice: x: 4, y: 4, z: 16, core: 2. Of those that a mesh axis runs over, the one named last changes fastest.
Arguments:
- tokens: bfloat16 [1024, 1024], P('ep'), may hold values from -6 to 6
- lengths: int32 [1024], P('ep'), may hold values from 1 to 512, as said below
- cache_keys: bfloat16 [1024, 512, 4, 128], P('ep', None, 'tp'), may hold values from -2.5 to 2.5
- cache_values: bfloat16 [1024, 512, 4, 128], P('ep', None, 'tp'), may hold values from -6 to 6
- cache_cum: float32 [1024, 4, 512], P('ep', 'tp'), may hold values from -1536 to 0, as said below
- norm_gain: bfloat16 [1024], replicated, may hold values from 0.099609375 to 1.8984375
- query_weight: bfloat16 [1024, 1024], P(None, 'tp'), may hold values from -0.1875 to 0.1875
- key_weight: bfloat16 [1024, 512], P(None, 'tp'), may hold values from -0.1875 to 0.1875
- value_weight: bfloat16 [1024, 512], P(None, 'tp'), may hold values from -0.1875 to 0.1875
- forget_weight: bfloat16 [1024, 4], P(None, 'tp'), may hold values from -0.1875 to 0.1875
- forget_bias: float32 [4], P('tp'), may hold values from -1 to 2
- query_gain: bfloat16 [128], replicated, may hold values from 0.29882812 to 2.5
- key_gain: bfloat16 [128], replicated, may hold values from 0.099609375 to 1.8984375
- out_weight: bfloat16 [1024, 1024], P('tp'), may hold values from -0.1875 to 0.1875
- ffn_gain: bfloat16 [1024], replicated, may hold values from 0.099609375 to 1.8984375
- mix_weight: bfloat16 [1024], replicated, may hold values from -0.1875 to 0.1875
- shared_gate: bfloat16 [1024, 4096], P(None, 'ep'), may hold values from -0.1875 to 0.1875
- shared_up: bfloat16 [1024, 4096], P(None, 'ep'), may hold values from -0.1875 to 0.1875
- shared_down: bfloat16 [4096, 1024], P('ep', 'tp'), may hold values from -0.09375 to 0.09375
- routes: int32 [1024, 2], P('ep'), may hold values from 0 to 127, all different within a row; in each aligned block of 8 rows (0 to 7, 8 to 15, ...) at most 4 rows name the same one
- route_weights: float32 [1024, 2], P('ep'), may hold values from 0.1 to 1
- expert_gate: bfloat16 [128, 1024, 512], P('ep', None, 'tp'), may hold values from -0.1875 to 0.1875
- expert_up: bfloat16 [128, 1024, 512], P('ep', None, 'tp'), may hold values from -0.1875 to 0.1875
- expert_down: bfloat16 [128, 512, 1024], P('ep', 'tp'), may hold values from -0.25 to 0.25
Outputs:
- layer_out: bfloat16 [1024, 1024], P('ep', 'tp')
The draws below stay inside these ranges and needn't reach their ends.
Inputs may be any that keep to these rules, and one draw needn't show every extreme that they name: `lengths`: at least one sequence has exactly 512 cached positions. `cache_cum`: along the positions each row never rises. `routes`: the 2 experts of a token differ; among the 8 rows of one device no expert is named by more than 4 rows, a bound that some block reaches.
All inputs are finite; a program needn't handle non-finite values.
Results may differ from the reference program's by a relative error of at most 0.013.
Values may be sent and summed in bfloat16 or wider, within the bound.
A program may use at most 64 MiB of HBM per device.

```python
import math
import jax
import jax.numpy as jnp
import numpy as np
from jax import lax

D = 1024
HEADS = 8
KV_HEADS = 4
HEAD = 128
FE = 512
FS = 4096
TOPK = 2
CAP = 4
SEQ_DEV = 8
CACHE = 512
SEQS = 1024
EXPERTS = 128
N_TP = 4


def draw_lengths(key, part):
    key_levels, key_lengths, key_chosen = jax.random.split(key, 3)
    blocks = SEQS // SEQ_DEV
    levels = jax.random.randint(key_levels, (blocks, 1), 1, 5)
    ceiling = CACHE * levels // 4
    drawn_lengths = jax.random.randint(key_lengths, (blocks, SEQ_DEV), 0, ceiling) + 1
    chosen = jax.random.randint(key_chosen, (), 0, SEQS)
    flat_lengths = drawn_lengths.reshape(-1)
    return jnp.where(jnp.arange(SEQS) == chosen, CACHE, flat_lengths).astype(jnp.int32)


def draw_cache_cum(key, part):
    key_slow, key_fast, key_seq, key_block, key_step = jax.random.split(key, 5)
    picks = jax.random.randint(key_slow, (SEQS, KV_HEADS, 1), 0, 10)
    slow_heads = picks < 5
    fast_span = float(min(30, max(CACHE // 8, 2)))
    fast_rate = 1.0 / jax.random.uniform(key_fast, (SEQS, KV_HEADS, 1), jnp.float32, fast_span, 2.0 * fast_span)
    decay_rate = jnp.where(slow_heads, 2.0 / CACHE, fast_rate)
    seq_factor = jnp.exp(jax.random.uniform(key_seq, (SEQS, 1, 1), jnp.float32, -0.69, 0.69))
    block_span = min(64, CACHE)
    block_factor = jax.random.uniform(key_block, (SEQS, KV_HEADS, CACHE // block_span, 1), jnp.float32, 0.5, 1.5)
    block_factor = jnp.broadcast_to(block_factor, (SEQS, KV_HEADS, CACHE // block_span, block_span))
    block_factor = block_factor.reshape(SEQS, KV_HEADS, CACHE)
    step_factor = jax.random.uniform(key_step, (SEQS, KV_HEADS, CACHE), jnp.float32, 0.5, 1.5)
    log_gate = -decay_rate * seq_factor * block_factor * step_factor
    return jnp.cumsum(log_gate, axis=-1).astype(jnp.float32)


def steps_of(rng, extent, shards, low, top_value):
    level = 1.0
    for dim, shards_of in shards:
        draws = jax.random.uniform(jax.random.fold_in(jax.random.fold_in(rng, 6), dim), (shards_of,), jnp.float32, low / len(shards), top_value / len(shards))
        level = level * jnp.repeat(jnp.exp(draws), extent[dim] // shards_of).reshape((-1,) + (1,) * (len(extent) - 1 - dim))
    return level


def shared_out(own_key, own, number, rows, amount, top, bound, skew):
    sequence = jax.random.permutation(own_key, amount)
    heavy_load, usual = load_shares(amount, rows * top, bound, skew, True), load_shares(amount, rows * top, bound, skew, False)
    places = jnp.arange(amount)

    def named(sizes, rotation):
        used = int((sizes > 0).sum())
        fixed = max(1, used // 4)
        moved = fixed + (places - fixed + rotation * (used - fixed)) % max(1, amount - fixed)
        return jnp.zeros((amount,), jnp.int32).at[sequence[jnp.where(places < fixed, places, moved)]].set(jnp.asarray(sizes, jnp.int32))

    sizes = jnp.where(number % 4 == 0, named(heavy_load, number // 4), named(usual, number - number // 4 - 1))
    mixed = jax.random.permutation(jax.random.fold_in(own, 3), amount)
    giver, taker = mixed[0:amount // 2 * 2:2], mixed[1:amount // 2 * 2:2]
    margin = jnp.minimum(sizes[giver] - 1, bound - sizes[taker]) // 2
    margin = jnp.where((giver == sequence[0]) | (taker == sequence[0]) | (sizes[taker] == 0), 0, jnp.maximum(margin, 0))
    moved = jax.random.randint(jax.random.fold_in(own, 4), (amount // 2,), 0, 1 << 20) % (margin + 1)
    sizes = sizes.at[giver].add(-moved).at[taker].add(moved)
    members = jnp.searchsorted(jnp.cumsum(sizes), jnp.arange(rows * top), side="right").astype(jnp.int32)
    grid = members.reshape(top, rows).T
    grid = grid[jax.random.permutation(jax.random.fold_in(own, 1), rows)]
    rotation = jax.random.randint(jax.random.fold_in(own, 2), (rows, 1), 0, top)
    return jnp.take_along_axis(grid, (jnp.arange(top)[None, :] + rotation) % top, axis=1)


def load_shares(number_of, total, reach, lean, full):
    portions = [(1 << 20) // math.isqrt(standing ** lean) + 1 for standing in range(1, number_of + 1)]
    largest = reach if full else min(reach, max(-(-total // number_of), total * portions[0] // sum(portions)))
    least = 1 if total - largest >= number_of - 1 else 0
    counts, spare = [largest] + [least] * (number_of - 1), total - largest - least * (number_of - 1)
    while spare > 0:
        movable = [i for i in range(1, number_of) if counts[i] < largest] or [i for i in range(1, number_of) if counts[i] < reach]
        whole, remaining = sum([portions[i] for i in movable]), spare
        for i in movable:
            more = min(reach - counts[i], max(1, remaining * portions[i] // whole), spare)
            counts[i] = counts[i] + more
            spare = spare - more
    return np.array(counts)


def normal_values(own_key, extent, width, limit, cuts=(), kind=jnp.bfloat16):
    factor_of = steps_of(own_key, extent, cuts, -0.22, 0.18) if cuts else 1.0
    array = jax.random.normal(own_key, extent, jnp.float32) * width * factor_of
    return jnp.minimum(jnp.maximum(array, -limit), limit).astype(kind)


def setup_inputs(seed: int = 0) -> dict:
    key_of = jax.random.split(jax.random.key(seed), 25)
    tokens = normal_values(key_of[0], (SEQS, D), 1.0, 6.0, ((0, 128),))
    lengths = draw_lengths(jax.random.fold_in(key_of[24], 71), 0)
    cache_keys = normal_values(key_of[2], (SEQS, CACHE, KV_HEADS, HEAD), 1.0, 2.5, ((0, 128), (2, 4)))
    cache_values = normal_values(key_of[3], (SEQS, CACHE, KV_HEADS, HEAD), 1.0, 6.0, ((0, 128), (2, 4)))
    cache_cum = draw_cache_cum(jax.random.fold_in(key_of[24], 71), 0)
    norm_gain = jnp.clip(1.0 + 0.18 * jax.random.normal(key_of[5], (D,), jnp.float32), 0.099609375, 1.8984375).astype(jnp.bfloat16)
    query_weight = normal_values(key_of[6], (D, HEADS * HEAD), D ** -0.5, 0.1875, ((1, 4),))
    key_weight = normal_values(key_of[7], (D, KV_HEADS * HEAD), D ** -0.5, 0.1875, ((1, 4),))
    value_weight = normal_values(key_of[8], (D, KV_HEADS * HEAD), D ** -0.5, 0.1875, ((1, 4),))
    forget_weight = normal_values(key_of[9], (D, KV_HEADS), D ** -0.5, 0.1875, ((1, 4),))
    forget_bias = jnp.clip(-1.0 + 3.0 * jax.random.uniform(key_of[10], (KV_HEADS,), jnp.float32) ** steps_of(key_of[10], (KV_HEADS,), ((0, 4),), -0.2, 0.2), -1.0, 2.0)
    query_gain = jnp.clip(jnp.exp(jax.random.uniform(key_of[11], (HEAD,), jnp.float32, math.log(0.29882812), math.log(2.5))), 0.29882812, 2.5).astype(jnp.bfloat16)
    key_gain = jnp.clip(1.0 + 0.18 * jax.random.normal(key_of[12], (HEAD,), jnp.float32), 0.099609375, 1.8984375).astype(jnp.bfloat16)
    out_weight = normal_values(key_of[13], (HEADS * HEAD, D), (HEADS * HEAD) ** -0.5, 0.1875, ((0, 4),))
    ffn_gain = jnp.clip(1.0 + 0.18 * jax.random.normal(key_of[14], (D,), jnp.float32), 0.099609375, 1.8984375).astype(jnp.bfloat16)
    mix_weight = normal_values(key_of[15], (D,), D ** -0.5, 0.1875)
    shared_gate = normal_values(key_of[16], (D, FS), D ** -0.5, 0.1875, ((1, 128),))
    shared_up = normal_values(key_of[17], (D, FS), D ** -0.5, 0.1875, ((1, 128),))
    shared_down = normal_values(key_of[18], (FS, D), FS ** -0.5, 0.09375, ((0, 128), (1, 4)))
    routes_keys = jax.random.split(jax.random.fold_in(key_of[19], 1), SEQS // SEQ_DEV)
    routes_turns = jax.random.permutation(jax.random.fold_in(key_of[19], 3), SEQS // SEQ_DEV)
    routes = jax.vmap(lambda own, number: shared_out(jax.random.fold_in(key_of[19], 2), own, number, SEQ_DEV, EXPERTS, TOPK, CAP, 2))(routes_keys, routes_turns).reshape((SEQS, TOPK))
    route_weights = jnp.clip(jnp.exp(math.log(1.0) - 2.3025851 * jax.random.uniform(key_of[20], (SEQS, TOPK), jnp.float32) ** steps_of(key_of[20], (SEQS, TOPK), ((0, 128),), -0.2, 0.2)), 0.1, 1.0)
    expert_gate = normal_values(key_of[21], (EXPERTS, D, FE), D ** -0.5, 0.1875, ((0, 128), (2, 4)))
    expert_up = normal_values(key_of[22], (EXPERTS, D, FE), D ** -0.5, 0.1875, ((0, 128), (2, 4)))
    expert_down = normal_values(key_of[23], (EXPERTS, FE, D), FE ** -0.5, 0.25, ((0, 128), (1, 4)))
    return dict(tokens=tokens, lengths=lengths, cache_keys=cache_keys, cache_values=cache_values, cache_cum=cache_cum, norm_gain=norm_gain, query_weight=query_weight, key_weight=key_weight, value_weight=value_weight, forget_weight=forget_weight, forget_bias=forget_bias, query_gain=query_gain, key_gain=key_gain, out_weight=out_weight, ffn_gain=ffn_gain, mix_weight=mix_weight, shared_gate=shared_gate, shared_up=shared_up, shared_down=shared_down, routes=routes, route_weights=route_weights, expert_gate=expert_gate, expert_up=expert_up, expert_down=expert_down)


epsilon = 1e-06

def rms_norm(values, gain):
    values = values.astype(jnp.float32)
    return values * lax.rsqrt(lax.optimization_barrier(jnp.mean(values * values, axis=-1, keepdims=True)) + epsilon) * gain.astype(jnp.float32)

def attend(inputs):
    query_one, key_one, value_one, log_one, keys_one, values_one, cum_one, length_one = inputs
    position = jnp.arange(CACHE, dtype=jnp.int32)
    live = position < length_one
    last_cum = lax.optimization_barrier(jnp.sum(jnp.where(position[None, :] == length_one - 1, cum_one, 0.0), axis=-1))
    gate_bias = last_cum[:, None] - cum_one + log_one[:, None]
    score_scale = HEAD ** (-0.5)
    past = jnp.einsum('kgd,pkd->kgp', query_one.astype(jnp.float32), keys_one.astype(jnp.float32)) * score_scale
    past = past + gate_bias[:, None, :]
    past = jnp.where(live[None, None, :], past, -jnp.inf)
    own = lax.optimization_barrier(jnp.sum(query_one.astype(jnp.float32) * key_one.astype(jnp.float32)[:, None, :], axis=-1)) * score_scale
    past_exp = jnp.exp(past)
    own_exp = jnp.exp(own)
    denominator = lax.optimization_barrier(jnp.sum(past_exp, axis=-1)) + own_exp
    past_prob = (past_exp / denominator[..., None]).astype(jnp.bfloat16)
    own_prob = (own_exp / denominator).astype(jnp.bfloat16)
    mixed = jnp.einsum('kgp,pkd->kgd', past_prob.astype(jnp.float32), values_one.astype(jnp.float32))
    mixed = mixed + own_prob.astype(jnp.float32)[..., None] * value_one.astype(jnp.float32)[:, None, :]
    return mixed.astype(jnp.bfloat16)

def reference(tokens, lengths, cache_keys, cache_values, cache_cum, norm_gain, query_weight, key_weight, value_weight, forget_weight, forget_bias, query_gain, key_gain, out_weight, ffn_gain, mix_weight, shared_gate, shared_up, shared_down, routes, route_weights, expert_gate, expert_up, expert_down):
    seq_count = tokens.shape[0]
    normed = rms_norm(tokens, norm_gain).astype(jnp.bfloat16)
    query = jnp.dot(normed, query_weight, preferred_element_type=jnp.float32)
    query = rms_norm(query.reshape(seq_count, KV_HEADS, HEADS // KV_HEADS, HEAD), query_gain).astype(jnp.bfloat16)
    new_key = jnp.dot(normed, key_weight, preferred_element_type=jnp.float32)
    new_key = rms_norm(new_key.reshape(seq_count, KV_HEADS, HEAD), key_gain).astype(jnp.bfloat16)
    new_value = jnp.dot(normed, value_weight, preferred_element_type=jnp.float32).astype(jnp.bfloat16)
    new_value = new_value.reshape(seq_count, KV_HEADS, HEAD)
    new_log = jax.nn.log_sigmoid(jnp.dot(normed, forget_weight, preferred_element_type=jnp.float32) + forget_bias)
    heads_out = lax.map(attend, (query, new_key, new_value, new_log, cache_keys, cache_values, cache_cum, lengths))
    heads_out = heads_out.reshape(seq_count, N_TP, -1)
    partial_value = jnp.einsum('btf,tfd->btd', heads_out.astype(jnp.float32), out_weight.reshape(N_TP, -1, D).astype(jnp.float32)).astype(jnp.bfloat16)
    attended = lax.optimization_barrier(jnp.sum(partial_value.astype(jnp.float32), axis=1))
    residual = tokens.astype(jnp.float32) + attended
    ffn_in = rms_norm(residual, ffn_gain).astype(jnp.bfloat16)
    mix_gate = jax.nn.sigmoid(jnp.dot(ffn_in, mix_weight, preferred_element_type=jnp.float32))
    pre_gate = jnp.dot(ffn_in, shared_gate, preferred_element_type=jnp.float32)
    pre_up = jnp.dot(ffn_in, shared_up, preferred_element_type=jnp.float32)
    shared_hidden = (jax.nn.silu(pre_gate) * pre_up).astype(jnp.bfloat16)
    dense = jnp.dot(shared_hidden, shared_down, preferred_element_type=jnp.float32)
    norm_weights = route_weights / lax.optimization_barrier(jnp.sum(route_weights, axis=1, keepdims=True))

    def expert_row(inputs):
        row, chosen, weights = inputs
        total = jnp.zeros((D,), jnp.float32)
        for route_slot in range(TOPK):
            index = chosen[route_slot]
            gate_mat = expert_gate[index]
            up_mat = expert_up[index]
            down_mat = expert_down[index]
            hidden = jax.nn.silu(jnp.dot(row, gate_mat, preferred_element_type=jnp.float32))
            hidden = (hidden * jnp.dot(row, up_mat, preferred_element_type=jnp.float32)).astype(jnp.bfloat16)
            parts = jnp.einsum('tf,tfd->td', hidden.reshape(N_TP, -1).astype(jnp.float32), down_mat.reshape(N_TP, -1, D).astype(jnp.float32)).astype(jnp.bfloat16)
            expert_out = lax.optimization_barrier(jnp.sum(parts.astype(jnp.float32), axis=0)).astype(jnp.bfloat16)
            total = total + weights[route_slot] * expert_out.astype(jnp.float32)
        return total
    routed = lax.map(expert_row, (ffn_in, routes, norm_weights))
    return (residual + mix_gate[:, None] * dense + routed).astype(jnp.bfloat16)
```

```python
import functools

import jax
import jax.numpy as jnp
from jax import lax
from jax.experimental import pallas as pl
from jax.experimental.pallas import tpu as pltpu
from jax.sharding import Mesh
from jax.sharding import PartitionSpec as P

MESH = pl.DeviceIdType.MESH
EP = ("z", "x", "c")
EPS = 1e-06
META = 128
BF = jnp.bfloat16
F32 = jnp.float32


def rms(values, gain):
    return values * lax.rsqrt(jnp.mean(values * values, axis=-1, keepdims=True) + EPS) * gain


def row_of(ref):
    return ref[...].astype(F32).reshape(1, -1)


def nt(a, b):
    return lax.dot_general(a, b, (((1,), (1,)), ((), ())), preferred_element_type=F32)


def mm(a, b):
    return jnp.dot(a, b, preferred_element_type=F32)


def silu(v):
    return v / (1.0 + jnp.exp(-v))


def hi_lo(v):
    hi = v.astype(BF).astype(F32)
    return hi, (v - hi).astype(BF).astype(F32)


def kernel(
    dims,
    tokens, lengths, cum, norm_gain, forget_w, forget_b, query_gain, key_gain, ffn_gain, mix_w,
    routes, route_w,
    keys_h, values_h, qw_h, kw_h, vw_h, ow_h, sg_h, su_h, sd_h, eg_h, eu_h, ed_h,
    out,
    keys, values, wqkv, ow, sg, su, wsd, wgu, wd,
    pt, zb, g, p3, rx1, s1, rx2, zs, rx3, ys, rx4,
    lsem, wsend, wrecv, fsend, frecv, tsend, trecv, zsend, zrecv, xsend, xrecv, csend, crecv,
    c2send, c2recv, x2send, x2recv, z2send, z2recv, ysend, yrecv,
):
    nz, nx, nc, nt_ = dims
    z, x, c, t = (lax.axis_index(a) for a in ("z", "x", "c", "t"))
    batch, depth = tokens.shape
    rows = batch // nt_
    head = keys.shape[2]
    cache = keys.shape[1]
    groups = qw_h.shape[1] // head
    width = depth // nt_
    hidden = eg_h.shape[1]
    strip = nz * rows

    def at(axis, base, step, size):
        return {axis: lax.rem(base + (step % size), size)}

    def idx(base, step, size):
        return lax.rem(base + (step % size), size)

    def rcopy(src, dst, ss, rs, dev):
        return pltpu.make_async_remote_copy(
            src_ref=src, dst_ref=dst, send_sem=ss, recv_sem=rs, device_id=dev, device_id_type=MESH
        )

    barrier = pltpu.get_barrier_semaphore()
    partners = (
        [at("t", t, d, nt_) for d in range(1, nt_)]
        + [at("c", c, d, nc) for d in range(1, nc)]
        + [at("x", x, d, nx) for d in range(1, nx)]
        + [at("z", z, d, nz) for d in range(1, nz)]
    )
    for dev in partners:
        pl.semaphore_signal(barrier, inc=1, device_id=dev, device_id_type=MESH)

    def local(i, src, dst):
        return pltpu.make_async_copy(src, dst, lsem.at[i])

    nq, nk = qw_h.shape[1], kw_h.shape[1]
    loads = [
        local(0, qw_h, wqkv.at[:, 0:nq]),
        local(1, kw_h, wqkv.at[:, nq : nq + nk]),
        local(2, vw_h, wqkv.at[:, nq + nk : nq + 2 * nk]),
        local(3, keys_h, keys),
        local(4, values_h, values),
        local(5, ow_h, ow),
        local(6, eg_h, wgu.at[t, :, 0:hidden]),
        local(7, eu_h, wgu.at[t, :, hidden : 2 * hidden]),
        local(8, ed_h, wd.at[t]),
        local(9, sd_h, wsd.at[t]),
        local(10, sg_h, sg),
        local(11, su_h, su),
    ]
    for cp in loads:
        cp.start()

    tok = tokens[...].astype(F32)
    normed = rms(tok, row_of(norm_gain)).astype(BF)
    logit = jnp.sum(normed.astype(F32) * forget_w[...].astype(F32), axis=-1, keepdims=True) + forget_b[0]
    new_log = jnp.minimum(logit, 0.0) - jnp.log(1.0 + jnp.exp(-jnp.abs(logit)))
    for i in (0, 1, 2):
        loads[i].wait()
    qkv = mm(normed, wqkv[...])
    qg, kg = row_of(query_gain), row_of(key_gain)
    q16 = jnp.concatenate(
        [rms(qkv[:, i * head : (i + 1) * head], qg).astype(BF) for i in range(groups)], axis=0
    )
    new_key = rms(qkv[:, nq : nq + nk], kg).astype(BF).astype(F32)
    new_value = qkv[:, nq + nk : nq + 2 * nk].astype(BF).astype(F32)
    new_key = jnp.concatenate([new_key] * groups, axis=0)
    new_value = jnp.concatenate([new_value] * groups, axis=0)

    n16 = batch * groups
    row16 = lax.rem(lax.broadcasted_iota(jnp.int32, (n16, cache), 0), batch)
    row8 = lax.broadcasted_iota(jnp.int32, (batch, cache), 0)
    pos8 = lax.broadcasted_iota(jnp.int32, (batch, cache), 1)
    length8 = jnp.zeros((batch, cache), jnp.int32)
    cum8 = jnp.zeros((batch, cache), F32)
    for s in range(batch):
        length8 = jnp.where(row8 == s, lengths[s], length8)
        cum8 = jnp.where(row8 == s, cum[s], cum8)
    last = jnp.sum(jnp.where(pos8 == length8 - 1, cum8, 0.0), axis=-1, keepdims=True)
    bias8 = last - cum8 + new_log
    bias8 = jnp.where(pos8 < length8, bias8, -jnp.inf)
    bias16 = jnp.concatenate([bias8] * groups, axis=0)
    loads[3].wait()
    scores = jnp.zeros((n16, cache), F32)
    for s in range(batch):
        scores = jnp.where(row16 == s, nt(q16, keys[s]), scores)
    scale = head ** (-0.5)
    past = jnp.exp(scores * scale + bias16)
    own = jnp.exp(jnp.sum(q16.astype(F32) * new_key, axis=-1, keepdims=True) * scale)
    denominator = jnp.sum(past, axis=-1, keepdims=True) + own
    prob = (past / denominator).astype(BF).astype(F32)
    own_prob = (own / denominator).astype(BF).astype(F32)
    loads[4].wait()
    mixed = own_prob * new_value
    for s in range(batch):
        mixed = mixed + mm(jnp.where(row16 == s, prob, 0.0).astype(BF), values[s])
    mixed = mixed.astype(BF)
    heads = jnp.concatenate([mixed[i * batch : (i + 1) * batch] for i in range(groups)], axis=1)
    loads[5].wait()
    partial = mm(heads, ow[...]).astype(BF)
    pt[t] = partial

    pl.semaphore_wait(barrier, len(partners))
    tsends = []
    for d in range(1, nt_):
        cp = rcopy(pt.at[t], pt.at[t], tsend.at[d], trecv.at[d], at("t", t, d, nt_))
        cp.start()
        tsends.append(cp)

    for i in (6, 7, 8, 9):
        loads[i].wait()
    half = depth // 2
    hhalf = ed_h.shape[0] // 2
    wsends = []
    for k, d in enumerate((1, nt_ - 1)):
        cps = [
            rcopy(wgu.at[t], wgu.at[t], wsend.at[k, 0], wrecv.at[k, 0], at("t", t, d, nt_)),
            rcopy(wd.at[t], wd.at[t], wsend.at[k, 1], wrecv.at[k, 1], at("t", t, d, nt_)),
            rcopy(wsd.at[t], wsd.at[t], wsend.at[k, 2], wrecv.at[k, 2], at("t", t, d, nt_)),
        ]
        for cp in cps:
            cp.start()
        wsends.append(cps)

    rowm = lax.broadcasted_iota(jnp.int32, (batch, META), 0)
    lane = lax.broadcasted_iota(jnp.int32, (batch, META), 1)
    zero = jnp.zeros((batch, META), F32)
    r0, r1, w0, w1 = zero, zero, zero, zero
    for s in range(batch):
        here = rowm == s
        r0 = jnp.where(here, routes[0, s].astype(F32), r0)
        r1 = jnp.where(here, routes[1, s].astype(F32), r1)
        w0 = jnp.where(here, route_w[0, s], w0)
        w1 = jnp.where(here, route_w[1, s], w1)
    total = w0 + w1
    h0, l0 = hi_lo(w0 / total)
    h1, l1 = hi_lo(w1 / total)

    residual = tok + pt[t].astype(F32)
    for d in range(1, nt_):
        peer = idx(t, nt_ - d, nt_)
        rcopy(pt.at[peer], pt.at[peer], tsend.at[d], trecv.at[d], at("t", t, d, nt_)).wait_recv()
        residual = residual + pt[peer].astype(F32)
    ffn = rms(residual, row_of(ffn_gain)).astype(BF).astype(F32)
    gate = jnp.sum(ffn * row_of(mix_w), axis=-1, keepdims=True)
    gate = 1.0 / (1.0 + jnp.exp(-gate))
    hg, lg = hi_lo(jnp.broadcast_to(gate, (batch, META)))
    meta = zero
    for i, v in enumerate((r0, r1, h0, l0, h1, l1, hg, lg)):
        meta = jnp.where(lane == i, v, meta)
    full = jnp.concatenate([ffn, meta], axis=1)

    def own_rows(v):
        sel = v[0:rows]
        for k in range(1, nt_):
            sel = jnp.where(t == k, v[k * rows : (k + 1) * rows], sel)
        return sel

    zb[z] = own_rows(full).astype(BF)
    zsends = []
    for d in sorted(range(1, nz), key=lambda d: -min(d, nz - d)):
        cp = rcopy(zb.at[z], zb.at[z], zsend.at[d], zrecv.at[d], at("z", z, d, nz))
        cp.start()
        zsends.append(cp)

    fsends = []

    def from_neighbour(k, part, ref, peer):
        rcopy(ref.at[peer], ref.at[peer], wsend.at[k, part], wrecv.at[k, part], at("t", t, 1, nt_)).wait_recv()

    left, right = idx(t, nt_ - 1, nt_), idx(t, 1, nt_)
    for d in range(1, nz):
        peer = idx(z, nz - d, nz)
        rcopy(zb.at[peer], zb.at[peer], zsend.at[d], zrecv.at[d], at("z", z, d, nz)).wait_recv()
    g[c, x] = zb[...].reshape(strip, depth + META)

    xsends = []
    for d in range(1, nx):
        cp = rcopy(g.at[c, x], g.at[c, x], xsend.at[d], xrecv.at[d], at("x", x, d, nx))
        cp.start()
        xsends.append(cp)
    twin = {"c": 1 - c}
    cp = rcopy(g.at[c, x], g.at[c, x], csend.at[0], crecv.at[0], twin)
    cp.start()
    xsends.append(cp)

    from_neighbour(0, 0, wgu, left)
    from_neighbour(1, 0, wgu, right)
    fsends += [
        rcopy(wgu.at[left, 0:half], wgu.at[left, 0:half], fsend.at[0, 0], frecv.at[0, 0], at("t", t, 1, nt_)),
        rcopy(wgu.at[right, half:depth], wgu.at[right, half:depth], fsend.at[1, 0], frecv.at[1, 0], at("t", t, nt_ - 1, nt_)),
    ]
    for cp in fsends:
        cp.start()

    for d in range(1, nx):
        peer = idx(x, nx - d, nx)
        rcopy(g.at[c, peer], g.at[c, peer], xsend.at[d], xrecv.at[d], at("x", x, d, nx)).wait_recv()
        cp = rcopy(g.at[c, peer], g.at[c, peer], csend.at[d], crecv.at[d], twin)
        cp.start()
        xsends.append(cp)
    for d in range(nx):
        peer = idx(x, nx - d, nx)
        rcopy(g.at[1 - c, peer], g.at[1 - c, peer], csend.at[d], crecv.at[d], twin).wait_recv()

    from_neighbour(0, 1, wd, left)
    from_neighbour(1, 1, wd, right)
    from_neighbour(0, 2, wsd, left)
    from_neighbour(1, 2, wsd, right)
    more = [
        rcopy(wd.at[left, 0:hhalf], wd.at[left, 0:hhalf], fsend.at[0, 1], frecv.at[0, 1], at("t", t, 1, nt_)),
        rcopy(wd.at[right, hhalf : 2 * hhalf], wd.at[right, hhalf : 2 * hhalf], fsend.at[1, 1], frecv.at[1, 1], at("t", t, nt_ - 1, nt_)),
        rcopy(wsd.at[left], wsd.at[left], fsend.at[0, 2], frecv.at[0, 2], at("t", t, 1, nt_)),
    ]
    for cp in more:
        cp.start()
    fsends += more

    total_rows = nc * nx * strip
    every = g[...].reshape(total_rows, depth + META)
    xs = every[:, 0:depth]
    info = every[:, depth : depth + META].astype(F32)
    mine = ((z * nx + x) * nc + c).astype(F32)
    w = jnp.where(info[:, 0:1] == mine, info[:, 2:3] + info[:, 3:4], 0.0)
    w = w + jnp.where(info[:, 1:2] == mine, info[:, 4:5] + info[:, 5:6], 0.0)
    mg = info[:, 6:7] + info[:, 7:8]

    loads[10].wait()
    loads[11].wait()
    sh = (silu(nt(xs, sg[...])) * nt(xs, su[...])).astype(BF)

    opp = idx(t, 2, nt_)
    hid = []
    for order in range(nt_):
        slot = idx(t, (0, 3, 1, 2)[order], nt_)
        if order == nt_ - 1:
            rcopy(wgu.at[opp, 0:half], wgu.at[opp, 0:half], fsend.at[0, 0], frecv.at[0, 0], at("t", t, 1, nt_)).wait_recv()
            rcopy(wgu.at[opp, half:depth], wgu.at[opp, half:depth], fsend.at[1, 0], frecv.at[1, 0], at("t", t, 1, nt_)).wait_recv()
        pre = mm(xs, wgu[slot])
        hid.append((silu(pre[:, 0:hidden]) * pre[:, hidden : 2 * hidden]).astype(BF))
    rcopy(wd.at[opp, 0:hhalf], wd.at[opp, 0:hhalf], fsend.at[0, 1], frecv.at[0, 1], at("t", t, 1, nt_)).wait_recv()
    rcopy(wd.at[opp, hhalf : 2 * hhalf], wd.at[opp, hhalf : 2 * hhalf], fsend.at[1, 1], frecv.at[1, 1], at("t", t, 1, nt_)).wait_recv()
    rcopy(wsd.at[opp], wsd.at[opp], fsend.at[0, 2], frecv.at[0, 2], at("t", t, 1, nt_)).wait_recv()
    res = mm(hid[0], wd[t])
    for order in range(1, nt_):
        res = res + mm(hid[order], wd[idx(t, (0, 3, 1, 2)[order], nt_)])
    dense = jnp.concatenate([mm(sh, wsd[k]) for k in range(nt_)], axis=1)
    p3[...] = (w * res + mg * dense).astype(BF).reshape(p3.shape)

    cp = rcopy(p3.at[1 - c], rx1, c2send, c2recv, twin)
    cp.start()
    ends = [cp]
    rcopy(p3.at[1 - c], rx1, c2send, c2recv, twin).wait_recv()
    for d in range(1, nx):
        peer = idx(x, d, nx)
        s1[peer] = (p3[c, peer].astype(F32) + rx1[peer].astype(F32)).astype(BF)
        cp = rcopy(s1.at[peer], rx2.at[d], x2send.at[d], x2recv.at[d], at("x", x, d, nx))
        cp.start()
        ends.append(cp)
    acc = p3[c, x].astype(F32) + rx1[x].astype(F32)
    for d in range(1, nx):
        rcopy(s1.at[x], rx2.at[d], x2send.at[d], x2recv.at[d], at("x", x, d, nx)).wait_recv()
        acc = acc + rx2[d].astype(F32)
    zs[...] = acc.astype(BF).reshape(nz, rows, depth)
    for d in sorted(range(1, nz), key=lambda d: -min(d, nz - d)):
        peer = idx(z, d, nz)
        cp = rcopy(zs.at[peer], rx3.at[d], z2send.at[d], z2recv.at[d], {"z": peer})
        cp.start()
        ends.append(cp)
    fin = zs[z].astype(F32)
    for d in range(1, nz):
        rcopy(zs.at[z], rx3.at[d], z2send.at[d], z2recv.at[d], at("z", z, d, nz)).wait_recv()
        fin = fin + rx3[d].astype(F32)

    spread = jnp.concatenate([fin] * nt_, axis=0)
    rowd = lax.broadcasted_iota(jnp.int32, (batch, depth), 0)
    spread = jnp.where((rowd >= t * rows) & (rowd < (t + 1) * rows), spread, 0.0)
    for k in range(nt_):
        ys[k] = spread[:, k * width : (k + 1) * width]
    for d in range(1, nt_):
        peer = idx(t, d, nt_)
        cp = rcopy(ys.at[peer], rx4.at[d], ysend.at[d], yrecv.at[d], {"t": peer})
        cp.start()
        ends.append(cp)
    result = residual[:, 0:width]
    for k in range(1, nt_):
        result = jnp.where(t == k, residual[:, k * width : (k + 1) * width], result)
    result = result + ys[t]
    for d in range(1, nt_):
        rcopy(ys.at[t], rx4.at[d], ysend.at[d], yrecv.at[d], at("t", t, d, nt_)).wait_recv()
        result = result + rx4[d]
    out[...] = result.astype(BF)

    for cp in tsends + zsends + xsends + fsends + ends + wsends[0] + wsends[1]:
        cp.wait_send()


def per_device(
    dims, tokens, lengths, cache_keys, cache_values, cache_cum, norm_gain, query_weight, key_weight,
    value_weight, forget_weight, forget_bias, query_gain, key_gain, out_weight, ffn_gain, mix_weight,
    shared_gate, shared_up, shared_down, routes, route_weights, expert_gate, expert_up, expert_down,
):
    nz, nx, nc, ny = dims
    batch, depth = tokens.shape
    cache, head = cache_keys.shape[1], cache_keys.shape[3]
    rows = batch // ny
    width = depth // ny
    strip = nz * rows
    hidden = expert_gate.shape[2]
    nq, nk = query_weight.shape[1], key_weight.shape[1]
    fs = shared_gate.shape[1]
    vm = pl.BlockSpec(memory_space=pltpu.VMEM)
    sm = pl.BlockSpec(memory_space=pltpu.SMEM)
    hb = pl.BlockSpec(memory_space=pltpu.HBM)
    dma = pltpu.SemaphoreType.DMA
    scratch = [
        pltpu.VMEM((batch, cache, head), BF),
        pltpu.VMEM((batch, cache, head), BF),
        pltpu.VMEM((depth, nq + 2 * nk), BF),
        pltpu.VMEM((nq, depth), BF),
        pltpu.VMEM((fs, depth), BF),
        pltpu.VMEM((fs, depth), BF),
        pltpu.VMEM((ny, fs, width), BF),
        pltpu.VMEM((ny, depth, 2 * hidden), BF),
        pltpu.VMEM((ny, hidden, depth), BF),
        pltpu.VMEM((ny, batch, depth), BF),
        pltpu.VMEM((nz, rows, depth + META), BF),
        pltpu.VMEM((nc, nx, strip, depth + META), BF),
        pltpu.VMEM((nc, nx, strip, depth), BF),
        pltpu.VMEM((nx, strip, depth), BF),
        pltpu.VMEM((nx, strip, depth), BF),
        pltpu.VMEM((nx, strip, depth), BF),
        pltpu.VMEM((nz, rows, depth), BF),
        pltpu.VMEM((nz, rows, depth), BF),
        pltpu.VMEM((ny, batch, width), F32),
        pltpu.VMEM((ny, batch, width), F32),
        dma((12,)),
        dma((2, 3)), dma((2, 3)), dma((2, 3)), dma((2, 3)),
        dma((ny,)), dma((ny,)), dma((nz,)), dma((nz,)), dma((nx,)), dma((nx,)), dma((nx,)), dma((nx,)),
        dma, dma, dma((nx,)), dma((nx,)), dma((nz,)), dma((nz,)), dma((ny,)), dma((ny,)),
    ]
    return pl.pallas_call(
        functools.partial(kernel, dims),
        out_shape=jax.ShapeDtypeStruct((batch, width), BF),
        in_specs=[vm, sm, vm, vm, vm, sm, vm, vm, vm, vm, sm, sm] + [hb] * 12,
        out_specs=vm,
        scratch_shapes=scratch,
        compiler_params=pltpu.CompilerParams(
            collective_id=0, has_side_effects=True, vmem_limit_bytes=48 * 1024 * 1024
        ),
    )(
        tokens, lengths, cache_cum, norm_gain, forget_weight.T, forget_bias, query_gain, key_gain,
        ffn_gain, mix_weight, routes.T, route_weights.T,
        cache_keys.reshape(batch, cache, head), cache_values.reshape(batch, cache, head),
        query_weight, key_weight, value_weight, out_weight, shared_gate.T, shared_up.T, shared_down,
        expert_gate[0], expert_up[0], expert_down[0],
    )


def solution(mesh):
    ep, ny = mesh.shape["ep"], mesh.shape["tp"]
    nz, nx, nc = (16, 4, 2) if ep == 128 else (ep // 4, 2, 2)
    finer = Mesh(mesh.devices.reshape(nz, nx, nc, ny), ("z", "x", "c", "t"))
    placed = (
        P(EP, None),
        P(EP),
        P(EP, None, "t", None),
        P(EP, None, "t", None),
        P(EP, "t", None),
        P(),
        P(None, "t"),
        P(None, "t"),
        P(None, "t"),
        P(None, "t"),
        P("t"),
        P(),
        P(),
        P("t", None),
        P(),
        P(),
        P(None, EP),
        P(None, EP),
        P(EP, "t"),
        P(EP, None),
        P(EP, None),
        P(EP, None, "t"),
        P(EP, None, "t"),
        P(EP, "t", None),
    )
    return jax.shard_map(
        functools.partial(per_device, (nz, nx, nc, ny)),
        mesh=finer, in_specs=placed, out_specs=P(EP, "t"), check_vma=False,
    )
```

```python
import functools

import jax
import jax.numpy as jnp
from jax import lax
from jax.experimental import pallas as pl
from jax.experimental.pallas import tpu as pltpu
from jax.sharding import Mesh
from jax.sharding import PartitionSpec as P

MESH = pl.DeviceIdType.MESH
EP = ("z", "x", "c")
EPS = 1e-06
META = 128
BF = jnp.bfloat16
NG = 2
F32 = jnp.float32


def rms(values, gain):
    return values * lax.rsqrt(jnp.mean(values * values, axis=-1, keepdims=True) + EPS) * gain


def row_of(ref):
    return ref[...].astype(F32).reshape(1, -1)


def nt(a, b):
    return lax.dot_general(a, b, (((1,), (1,)), ((), ())), preferred_element_type=F32)


def mm(a, b):
    return jnp.dot(a, b, preferred_element_type=F32)


def silu(v):
    return v / (1.0 + jnp.exp(-v))


class Phases:
    def __init__(self):
        self.open = None

    def __call__(self, name):
        self.close()
        self.open = jax.named_scope(name)
        self.open.__enter__()

    def close(self):
        if self.open is not None:
            self.open.__exit__(None, None, None)
            self.open = None


def hi_lo(v):
    hi = v.astype(BF).astype(F32)
    return hi, (v - hi).astype(BF).astype(F32)


def kernel(
    dims,
    tokens_h, lengths_h, cum_h, norm_gain_h, forget_w_h, forget_b_h, query_gain_h, key_gain_h, ffn_gain_h,
    mix_w_h, routes_h, route_w_h,
    keys_h, values_h, qw_h, kw_h, vw_h, ow_h, sg_h, su_h, sd_h, eg_h, eu_h, ed_h,
    out,
    tokens, lengths, cum, norm_gain, forget_w, forget_b, query_gain, key_gain, ffn_gain, mix_w,
    routes, route_w,
    keys, values, wqkv, ow, sg, su, wsd, wgu, wd,
    pt, zb, g, p3, rx1, s1, rx2, zs, rx3,
    known, lsem, wsend, wrecv, tsend, trecv, zsend, zrecv, xsend, xrecv, csend, crecv, ysend, yrecv,
    c2send, c2recv, x2send, x2recv, z2send, z2recv,
):
    nz, nx, nc, nt_ = dims
    phase = Phases()
    z, x, c, t = (lax.axis_index(a) for a in ("z", "x", "c", "t"))
    batch, depth = tokens.shape
    rows = batch // nt_
    head = keys.shape[2]
    cache = keys.shape[1]
    groups = qw_h.shape[1] // head
    width = depth // nt_
    hidden = eg_h.shape[1]
    wide = depth + META
    near = nz // NG
    strip = near * rows
    part_rows = nx * 2 * strip
    order = sorted(range(nz), key=lambda d: (min(d, nz - d), d))
    place = [order.index(d) for d in range(nz)]

    def idx(base, step, size):
        return lax.rem(base + (step % size), size)

    def at(axis, base, step, size):
        return {axis: idx(base, step, size)}

    def rcopy(src, dst, ss, rs, dev):
        return pltpu.make_async_remote_copy(
            src_ref=src, dst_ref=dst, send_sem=ss, recv_sem=rs, device_id=dev, device_id_type=MESH
        )

    def send(*args):
        rcopy(*args).start()

    def landed(ref, sem):
        pltpu.make_async_copy(ref, ref, sem).wait()

    phase("entry")
    barrier = pltpu.get_barrier_semaphore()
    partners = (
        [at("t", t, d, nt_) for d in range(1, nt_)]
        + [at("c", c, d, nc) for d in range(1, nc)]
        + [at("x", x, d, nx) for d in range(1, nx)]
        + [at("z", z, d, nz) for d in range(1, nz) if min(d, nz - d) <= nz // 4]
    )
    for dev in partners:
        pl.semaphore_signal(barrier, inc=1, device_id=dev, device_id_type=MESH)

    def local(i, src, dst):
        return pltpu.make_async_copy(src, dst, lsem.at[i])

    nq, nk = qw_h.shape[1], kw_h.shape[1]
    loads = [
        local(0, qw_h, wqkv.at[:, 0:nq]),
        local(0, kw_h, wqkv.at[:, nq : nq + nk]),
        local(0, vw_h, wqkv.at[:, nq + nk : nq + 2 * nk]),
        local(3, keys_h, keys),
        local(4, values_h, values),
        local(5, ow_h, ow),
        local(6, eg_h, wgu.at[0, :, 0:hidden]),
        local(6, eu_h, wgu.at[0, :, hidden : 2 * hidden]),
        local(8, ed_h, wd.at[0]),
        local(9, sd_h, wsd.at[t]),
        local(10, sg_h, sg),
        local(11, su_h, su),
    ]
    small = [
        local(12 + i, src, dst)
        for i, (src, dst) in enumerate((
            (tokens_h, tokens), (norm_gain_h, norm_gain), (forget_w_h, forget_w), (forget_b_h, forget_b),
            (query_gain_h, query_gain), (key_gain_h, key_gain), (lengths_h, lengths), (cum_h, cum),
            (ffn_gain_h, ffn_gain), (mix_w_h, mix_w), (routes_h, routes), (route_w_h, route_w),
        ))
    ]
    for cp in small + loads:
        cp.start()
    phase("small_wait")
    for cp in small:
        cp.wait()

    opp = idx(t, 2, nt_)
    partner = lax.rem(t + 1 + 2 * lax.rem(t + c, 2), nt_)
    wsd[opp] = jnp.zeros(wsd.shape[1:], BF)
    wsd[idx(partner, 2, nt_)] = jnp.zeros(wsd.shape[1:], BF)

    phase("norm")
    tok = tokens[...].astype(F32)
    normed = rms(tok, row_of(norm_gain)).astype(BF)
    logit = jnp.sum(normed.astype(F32) * forget_w[...].astype(F32), axis=-1, keepdims=True) + forget_b[...]
    new_log = jnp.minimum(logit, 0.0) - jnp.log(1.0 + jnp.exp(-jnp.abs(logit)))
    landed(wqkv, lsem.at[0])
    phase("qkv")
    qkv = mm(normed, wqkv[...])
    qg, kg = row_of(query_gain), row_of(key_gain)
    q16 = jnp.concatenate(
        [rms(qkv[:, i * head : (i + 1) * head], qg).astype(BF) for i in range(groups)], axis=0
    )
    new_key = rms(qkv[:, nq : nq + nk], kg).astype(BF).astype(F32)
    new_value = qkv[:, nq + nk : nq + 2 * nk].astype(BF).astype(F32)
    new_key = jnp.concatenate([new_key] * groups, axis=0)
    new_value = jnp.concatenate([new_value] * groups, axis=0)
    phase("bias")
    n16 = batch * groups
    row16 = lax.rem(lax.broadcasted_iota(jnp.int32, (n16, cache), 0), batch)
    row8 = lax.broadcasted_iota(jnp.int32, (batch, cache), 0)
    pos8 = lax.broadcasted_iota(jnp.int32, (batch, cache), 1)
    length8 = jnp.zeros((batch, cache), jnp.int32)
    cum8 = jnp.zeros((batch, cache), F32)
    for s in range(batch):
        length8 = jnp.where(row8 == s, lengths[s], length8)
        cum8 = jnp.where(row8 == s, cum[s], cum8)
    last = jnp.sum(jnp.where(pos8 == length8 - 1, cum8, 0.0), axis=-1, keepdims=True)
    bias8 = last - cum8 + new_log
    bias8 = jnp.where(pos8 < length8, bias8, -jnp.inf)
    bias16 = jnp.concatenate([bias8] * groups, axis=0)
    loads[3].wait()
    phase("scores")
    scores = jnp.zeros((n16, cache), F32)
    for s in range(batch):
        scores = jnp.where(row16 == s, nt(q16, keys[s]), scores)
    phase("softmax")
    scale = head ** (-0.5)
    past = jnp.exp(scores * scale + bias16)
    own = jnp.exp(jnp.sum(q16.astype(F32) * new_key, axis=-1, keepdims=True) * scale)
    denominator = jnp.sum(past, axis=-1, keepdims=True) + own
    prob = (past / denominator).astype(BF).astype(F32)
    own_prob = (own / denominator).astype(BF).astype(F32)
    loads[4].wait()
    phase("values")
    mixed = own_prob * new_value
    for s in range(batch):
        mixed = mixed + mm(jnp.where(row16 == s, prob, 0.0).astype(BF), values[s])
    mixed = mixed.astype(BF)
    loads[5].wait()
    phase("outproj")
    heads = jnp.concatenate([mixed[i * batch : (i + 1) * batch] for i in range(groups)], axis=1)
    partial = mm(heads, ow[...]).astype(BF)
    pt[0] = partial

    phase("barrier")
    pl.semaphore_wait(barrier, len(partners))
    for d in (nz // 4, nz - nz // 4):
        pl.semaphore_signal(known, inc=1, device_id=at("z", z, d, nz), device_id_type=MESH)
    phase("tsend")
    for d in (2, 1, 3):
        send(pt.at[0], pt.at[d], tsend, trecv, at("t", t, d, nt_))

    landed(wgu.at[0], lsem.at[6])
    loads[8].wait()
    loads[9].wait()
    there = {"t": partner}
    send(wgu.at[0], wgu.at[1], wsend.at[0], wrecv.at[0], there)
    send(wd.at[0], wd.at[1], wsend.at[1], wrecv.at[1], there)
    send(wsd.at[t], wsd.at[t], wsend.at[2], wrecv.at[2], there)

    phase("route")
    rowm = lax.broadcasted_iota(jnp.int32, (batch, META), 0)
    lane = lax.broadcasted_iota(jnp.int32, (batch, META), 1)
    zero = jnp.zeros((batch, META), F32)
    r0, r1, w0, w1 = zero, zero, zero, zero
    for s in range(batch):
        here = rowm == s
        r0 = jnp.where(here, routes[0, s].astype(F32), r0)
        r1 = jnp.where(here, routes[1, s].astype(F32), r1)
        w0 = jnp.where(here, route_w[0, s], w0)
        w1 = jnp.where(here, route_w[1, s], w1)
    total = w0 + w1
    h0, l0 = hi_lo(w0 / total)
    h1, l1 = hi_lo(w1 / total)
    for i in (10, 11):
        loads[i].wait()

    phase("twait")
    landed(pt.at[1:nt_], trecv)
    residual = tok + pt[0].astype(F32)
    for d in range(1, nt_):
        residual = residual + pt[d].astype(F32)
    phase("ffn")
    ffn = rms(residual, row_of(ffn_gain)).astype(BF).astype(F32)
    gate = jnp.sum(ffn * row_of(mix_w), axis=-1, keepdims=True)
    gate = 1.0 / (1.0 + jnp.exp(-gate))
    hg, lg = hi_lo(jnp.broadcast_to(gate, (batch, META)))
    meta = zero
    for i, v in enumerate((r0, r1, h0, l0, h1, l1, hg, lg)):
        meta = jnp.where(lane == i, v, meta)
    full = jnp.concatenate([ffn, meta], axis=1)
    sel = full[0:rows]
    for k in range(1, nt_):
        sel = jnp.where(t == k, full[k * rows : (k + 1) * rows], sel)
    zb[0] = sel.astype(BF)
    mine8 = residual[:, 0:width]
    for k in range(1, nt_):
        mine8 = jnp.where(t == k, residual[:, k * width : (k + 1) * width], mine8)

    phase("spread2")
    pl.semaphore_wait(known, 2)
    phase("zsend")
    for d in order[:0:-1]:
        send(zb.at[0], zb.at[place[d]], zsend, zrecv.at[place[d] // near], at("z", z, d, nz))

    twin = {"c": 1 - c}
    level = lax.div(t, 2)

    def spot(dx, dq):
        return 2 * idx(x, dx, nx) + (1 - level if dq else level)

    def place_of(dx, dq):
        return {"x": idx(x, dx, nx), "t": idx(t, 2 * dq, nt_)}

    far_first = [(2, 1), (2, 0), (1, 1), (3, 1), (0, 1), (1, 0), (3, 0)]
    me = spot(0, 0)

    def take_z(h):
        phase("zwait#h=%d" % h)
        landed(zb.at[max(1, h * near) : (h + 1) * near], zrecv.at[h])
        phase("xsend#h=%d" % h)
        g[h, c, me] = zb[h * near : (h + 1) * near].reshape(strip, wide)
        piece = g.at[h, c, me]
        send(piece, piece, ysend, yrecv.at[h], {"t": opp})
        hand_on(h, 0)

    def hand_on(h, dq):
        piece = g.at[h, c, spot(0, dq)]
        for dx in (2, 1, 3):
            send(piece, piece, xsend.at[h], xrecv.at[h, dq, dx], at("x", x, dx, nx))
        send(piece, piece, csend.at[h], crecv.at[h], twin)

    def take_y(h):
        phase("yfwd#h=%d" % h)
        landed(g.at[h, c, spot(0, 1)], yrecv.at[h])
        hand_on(h, 1)

    def take_x(h, dq):
        phase("xwait%d#h=%d" % (dq, h))
        for dx in (1, 3, 2):
            piece = g.at[h, c, spot(nx - dx, dq)]
            landed(piece, xrecv.at[h, dq, dx])
            send(piece, piece, csend.at[h], crecv.at[h], twin)

    def take_c(h):
        phase("cwait#h=%d" % h)
        landed(g.at[h, 1 - c], crecv.at[h])

    mine = ((z * nx + x) * nc + c).astype(F32)

    def compute(h, core, name):
        phase("%s#h=%d" % (name, h))
        every = g[h, core].reshape(part_rows, wide)
        info = every[:, depth:wide].astype(F32)
        w = jnp.where(info[:, 0:1] == mine, info[:, 2:3] + info[:, 3:4], 0.0)
        w = w + jnp.where(info[:, 1:2] == mine, info[:, 4:5] + info[:, 5:6], 0.0)
        xs = every[:, 0:depth]
        hid = []
        for k in (0, 1):
            pre = mm(xs, wgu[k])
            hid.append((silu(pre[:, 0:hidden]) * pre[:, hidden : 2 * hidden]).astype(BF))
        sh = (silu(nt(xs, sg[...])) * nt(xs, su[...])).astype(BF)
        dense = jnp.concatenate([mm(sh, wsd[k]) for k in range(nt_)], axis=1)
        res = mm(jnp.concatenate(hid, axis=1), wd[...].reshape(2 * hidden, depth))
        value = w * res + (info[:, 6:7] + info[:, 7:8]) * dense
        p3[h, core] = value.astype(BF).reshape(2 * nx, strip, depth)

    def send_c(h):
        send(p3.at[h, 1 - c], rx1.at[h], c2send.at[h], c2recv.at[h], twin)

    def sum_c(h):
        phase("c2#h=%d" % h)
        landed(rx1.at[h], c2recv.at[h])
        for dx, dq in far_first:
            at_ = spot(dx, dq)
            s1[h, at_] = (p3[h, c, at_].astype(F32) + rx1[h, at_].astype(F32)).astype(BF)
            send(s1.at[h, at_], rx2.at[h, 2 * dx + dq], x2send.at[h], x2recv.at[h], place_of(dx, dq))

    def sum_x(h):
        phase("x2#h=%d" % h)
        acc = p3[h, c, me].astype(F32) + rx1[h, me].astype(F32)
        landed(rx2.at[h, 1 : 2 * nx], x2recv.at[h])
        for i in range(1, 2 * nx):
            acc = acc + rx2[h, i].astype(F32)
        phase("z2send#h=%d" % h)
        for k in range(nt_):
            zs[h, k * near : (k + 1) * near] = acc[:, k * width : (k + 1) * width].astype(BF).reshape(near, rows, width)
        for d in order[h * near : (h + 1) * near][::-1]:
            i = place[d] - h * near
            for e in (2, 1, 3, 0):
                if d or e:
                    peer = idx(t, e, nt_)
                    send(zs.at[h, peer * near + i], rx3.at[t, d], z2send.at[h], z2recv.at[t], {"z": idx(z, nz - d, nz), "t": peer})
                else:
                    rx3[t, 0] = zs[0, t * near]

    take_z(0)
    take_z(1)
    take_y(0)
    take_x(0, 0)
    take_y(1)
    take_x(0, 1)
    phase("wwait")
    landed(wgu.at[1], wrecv.at[0])
    landed(wd.at[1], wrecv.at[1])
    landed(wsd.at[partner], wrecv.at[2])
    compute(0, c, "own")
    take_x(1, 0)
    take_c(0)
    compute(0, 1 - c, "twin")
    send_c(0)
    take_x(1, 1)
    compute(1, c, "own")
    sum_c(0)
    take_c(1)
    compute(1, 1 - c, "twin")
    send_c(1)
    sum_c(NG - 1)
    for h in range(NG):
        sum_x(h)
    phase("z2wait")
    for e in range(nt_):
        k = idx(t, e, nt_)
        landed(rx3.at[k] if e else rx3.at[k, 1:nz], z2recv.at[k])
    phase("result")
    sums = [jnp.sum(rx3[k].astype(F32), axis=0) for k in range(nt_)]
    out[...] = mine8 + jnp.concatenate(sums, axis=0)

    phase("drain")
    landed(pt.at[1:nt_], tsend)
    landed(zb.at[1:nz], zsend)
    landed(wgu.at[0], wsend.at[0])
    landed(wd.at[0], wsend.at[1])
    landed(wsd.at[0], wsend.at[2])
    landed(g.at[0, 0, 0:NG], ysend)
    for h in range(NG):
        landed(g.at[h, 0, 2 : 2 * nx], xsend.at[h])
        landed(g.at[h, 0], csend.at[h])
        landed(rx1.at[h], c2send.at[h])
        landed(rx2.at[h, 1 : 2 * nx], x2send.at[h])
        landed(zs.at[h] if h else zs.at[h, 1 : nt_ * near], z2send.at[h])
    phase.close()


def per_device(
    dims, tokens, lengths, cache_keys, cache_values, cache_cum, norm_gain, query_weight, key_weight,
    value_weight, forget_weight, forget_bias, query_gain, key_gain, out_weight, ffn_gain, mix_weight,
    shared_gate, shared_up, shared_down, routes, route_weights, expert_gate, expert_up, expert_down,
):
    nz, nx, nc, ny = dims
    batch, depth = tokens.shape
    cache, head = cache_keys.shape[1], cache_keys.shape[3]
    rows = batch // ny
    width = depth // ny
    strip = nz // NG * rows
    hidden = expert_gate.shape[2]
    nq, nk = query_weight.shape[1], key_weight.shape[1]
    fs = shared_gate.shape[1]
    vm = pl.BlockSpec(memory_space=pltpu.VMEM)
    hb = pl.BlockSpec(memory_space=pltpu.HBM)
    dma = pltpu.SemaphoreType.DMA
    scratch = [
        pltpu.VMEM((batch, depth), BF),
        pltpu.SMEM((batch,), jnp.int32),
        pltpu.VMEM((batch, 1, cache), F32),
        pltpu.VMEM((depth,), BF),
        pltpu.VMEM((1, depth), BF),
        pltpu.VMEM((1, 1), F32),
        pltpu.VMEM((head,), BF),
        pltpu.VMEM((head,), BF),
        pltpu.VMEM((depth,), BF),
        pltpu.VMEM((depth,), BF),
        pltpu.SMEM((routes.shape[1], batch), jnp.int32),
        pltpu.SMEM((routes.shape[1], batch), F32),
        pltpu.VMEM((batch, cache, head), BF),
        pltpu.VMEM((batch, cache, head), BF),
        pltpu.VMEM((depth, nq + 2 * nk), BF),
        pltpu.VMEM((nq, depth), BF),
        pltpu.VMEM((fs, depth), BF),
        pltpu.VMEM((fs, depth), BF),
        pltpu.VMEM((ny, fs, width), BF),
        pltpu.VMEM((2, depth, 2 * hidden), BF),
        pltpu.VMEM((2, hidden, depth), BF),
        pltpu.VMEM((ny, batch, depth), BF),
        pltpu.VMEM((nz, rows, depth + META), BF),
        pltpu.VMEM((NG, nc, 2 * nx, strip, depth + META), BF),
        pltpu.VMEM((NG, nc, 2 * nx, strip, depth), BF),
        pltpu.VMEM((NG, 2 * nx, strip, depth), BF),
        pltpu.VMEM((NG, 2 * nx, strip, depth), BF),
        pltpu.VMEM((NG, 2 * nx, strip, depth), BF),
        pltpu.VMEM((NG, ny * (nz // NG), rows, width), BF),
        pltpu.VMEM((ny, nz, rows, width), BF),
        pltpu.SemaphoreType.REGULAR,
        dma((24,)),
        dma((3,)), dma((3,)),
        dma, dma, dma, dma((NG,)), dma((NG,)), dma((NG, 2, nx)), dma((NG,)), dma((NG,)), dma, dma((NG,)),
        dma((NG,)), dma((NG,)), dma((NG,)), dma((NG,)), dma((NG,)), dma((ny,)),
    ]
    return pl.pallas_call(
        functools.partial(kernel, dims),
        out_shape=jax.ShapeDtypeStruct((batch, width), F32),
        in_specs=[hb] * 24,
        out_specs=vm,
        scratch_shapes=scratch,
        compiler_params=pltpu.CompilerParams(
            collective_id=0, has_side_effects=True, vmem_limit_bytes=60 * 1024 * 1024
        ),
    )(
        tokens, lengths, cache_cum, norm_gain, forget_weight.T, forget_bias.reshape(1, 1), query_gain, key_gain,
        ffn_gain, mix_weight, routes.T, route_weights.T,
        cache_keys.reshape(batch, cache, head), cache_values.reshape(batch, cache, head),
        query_weight, key_weight, value_weight, out_weight, shared_gate.T, shared_up.T, shared_down,
        expert_gate[0], expert_up[0], expert_down[0],
    ).astype(BF)


def solution(mesh):
    ep, ny = mesh.shape["ep"], mesh.shape["tp"]
    nz, nx, nc = (16, 4, 2) if ep == 128 else (ep // 4, 2, 2)
    finer = Mesh(mesh.devices.reshape(nz, nx, nc, ny), ("z", "x", "c", "t"))
    placed = (
        P(EP, None),
        P(EP),
        P(EP, None, "t", None),
        P(EP, None, "t", None),
        P(EP, "t", None),
        P(),
        P(None, "t"),
        P(None, "t"),
        P(None, "t"),
        P(None, "t"),
        P("t"),
        P(),
        P(),
        P("t", None),
        P(),
        P(),
        P(None, EP),
        P(None, EP),
        P(EP, "t"),
        P(EP, None),
        P(EP, None),
        P(EP, None, "t"),
        P(EP, None, "t"),
        P(EP, "t", None),
    )
    return jax.shard_map(
        functools.partial(per_device, (nz, nx, nc, ny)),
        mesh=finer, in_specs=placed, out_specs=P(EP, "t"), check_vma=False,
    )
```

```python
import functools

import jax
import jax.numpy as jnp
from jax import lax
from jax.experimental import pallas as pl
from jax.experimental.pallas import tpu as pltpu
from jax.sharding import Mesh
from jax.sharding import PartitionSpec as P

MESH = pl.DeviceIdType.MESH
EP = ("z", "x", "c")
EPS = 1e-06
META = 128
BF = jnp.bfloat16
NG = 4
F32 = jnp.float32


def rms(values, gain):
    return values * lax.rsqrt(jnp.mean(values * values, axis=-1, keepdims=True) + EPS) * gain


def row_of(ref):
    return ref[...].astype(F32).reshape(1, -1)


def nt(a, b):
    return lax.dot_general(a, b, (((1,), (1,)), ((), ())), preferred_element_type=F32)


def mm(a, b):
    return jnp.dot(a, b, preferred_element_type=F32)


def silu(v):
    return v / (1.0 + jnp.exp(-v))


class Phases:
    def __init__(self):
        self.open = None

    def __call__(self, name):
        self.close()
        self.open = jax.named_scope(name)
        self.open.__enter__()

    def close(self):
        if self.open is not None:
            self.open.__exit__(None, None, None)
            self.open = None


def hi_lo(v):
    hi = v.astype(BF).astype(F32)
    return hi, (v - hi).astype(BF).astype(F32)


def kernel(
    dims,
    tokens_h, lengths_h, cum_h, norm_gain_h, forget_w_h, forget_b_h, query_gain_h, key_gain_h, ffn_gain_h,
    mix_w_h, routes_h, route_w_h,
    keys_h, values_h, qw_h, kw_h, vw_h, ow_h, sg_h, su_h, sd_h, eg_h, eu_h, ed_h,
    out,
    tokens, lengths, cum, norm_gain, forget_w, forget_b, query_gain, key_gain, ffn_gain, mix_w,
    routes, route_w,
    keys, values, wqkv, ow, sg, su, wsd, wgu, wd,
    pt, ob, zb, g, p3, rx1, s1, rx2, zs, rx3,
    known, lsem, wsend, wrecv, tsend, trecv, zsend, zrecv, xsend, xrecv, csend, crecv, ysend, yrecv,
    c2send, c2recv, x2send, x2recv, z2send, z2recv,
):
    nz, nx, nc, nt_ = dims
    phase = Phases()
    z, x, c, t = (lax.axis_index(a) for a in ("z", "x", "c", "t"))
    batch, depth = tokens.shape
    rows = batch // nt_
    head = keys.shape[2]
    cache = keys.shape[1]
    groups = qw_h.shape[1] // head
    width = depth // nt_
    hidden = eg_h.shape[1]
    wide = depth + META
    near = nz // NG
    strip = near * rows
    part_rows = nx * 2 * strip
    def idx(base, step, size):
        return lax.rem(base + (step % size), size)

    def at(axis, base, step, size):
        return {axis: idx(base, step, size)}

    def rcopy(src, dst, ss, rs, dev):
        return pltpu.make_async_remote_copy(
            src_ref=src, dst_ref=dst, send_sem=ss, recv_sem=rs, device_id=dev, device_id_type=MESH
        )

    def send(*args):
        rcopy(*args).start()

    def landed(ref, sem):
        pltpu.make_async_copy(ref, ref, sem).wait()

    phase("entry")
    barrier = pltpu.get_barrier_semaphore()
    partners = (
        [at("t", t, d, nt_) for d in range(1, nt_)]
        + [at("c", c, d, nc) for d in range(1, nc)]
        + [at("x", x, d, nx) for d in range(1, nx)]
        + [at("z", z, d, nz) for d in range(1, nz) if min(d, nz - d) <= nz // 4]
    )
    for dev in partners:
        pl.semaphore_signal(barrier, inc=1, device_id=dev, device_id_type=MESH)

    def local(i, src, dst):
        return pltpu.make_async_copy(src, dst, lsem.at[i])

    nq, nk = qw_h.shape[1], kw_h.shape[1]
    loads = [
        local(0, qw_h, wqkv.at[:, 0:nq]),
        local(0, kw_h, wqkv.at[:, nq : nq + nk]),
        local(0, vw_h, wqkv.at[:, nq + nk : nq + 2 * nk]),
        local(3, keys_h, keys),
        local(4, values_h, values),
        local(5, ow_h, ow),
        local(6, eg_h, wgu.at[0, :, 0:hidden]),
        local(6, eu_h, wgu.at[0, :, hidden : 2 * hidden]),
        local(8, ed_h, wd.at[0]),
        local(9, sd_h, wsd.at[t]),
        local(10, sg_h, sg),
        local(11, su_h, su),
    ]
    small = [
        local(12 + i, src, dst)
        for i, (src, dst) in enumerate((
            (tokens_h, tokens), (norm_gain_h, norm_gain), (forget_w_h, forget_w), (forget_b_h, forget_b),
            (query_gain_h, query_gain), (key_gain_h, key_gain), (lengths_h, lengths), (cum_h, cum),
            (ffn_gain_h, ffn_gain), (mix_w_h, mix_w), (routes_h, routes), (route_w_h, route_w),
        ))
    ]
    for cp in small + loads:
        cp.start()
    phase("small_wait")
    for cp in small:
        cp.wait()

    opp = idx(t, 2, nt_)
    partner = lax.rem(t + 1 + 2 * lax.rem(t + c, 2), nt_)
    wsd[opp] = jnp.zeros(wsd.shape[1:], BF)
    wsd[idx(partner, 2, nt_)] = jnp.zeros(wsd.shape[1:], BF)

    phase("norm")
    tok = tokens[...].astype(F32)
    normed = rms(tok, row_of(norm_gain)).astype(BF)
    logit = jnp.sum(normed.astype(F32) * forget_w[...].astype(F32), axis=-1, keepdims=True) + forget_b[...]
    new_log = jnp.minimum(logit, 0.0) - jnp.log(1.0 + jnp.exp(-jnp.abs(logit)))
    landed(wqkv, lsem.at[0])
    phase("qkv")
    qkv = mm(normed, wqkv[...])
    qg, kg = row_of(query_gain), row_of(key_gain)
    q16 = jnp.concatenate(
        [rms(qkv[:, i * head : (i + 1) * head], qg).astype(BF) for i in range(groups)], axis=0
    )
    new_key = rms(qkv[:, nq : nq + nk], kg).astype(BF).astype(F32)
    new_value = qkv[:, nq + nk : nq + 2 * nk].astype(BF).astype(F32)
    new_key = jnp.concatenate([new_key] * groups, axis=0)
    new_value = jnp.concatenate([new_value] * groups, axis=0)
    phase("bias")
    n16 = batch * groups
    row16 = lax.rem(lax.broadcasted_iota(jnp.int32, (n16, cache), 0), batch)
    row8 = lax.broadcasted_iota(jnp.int32, (batch, cache), 0)
    pos8 = lax.broadcasted_iota(jnp.int32, (batch, cache), 1)
    length8 = jnp.zeros((batch, cache), jnp.int32)
    cum8 = jnp.zeros((batch, cache), F32)
    for s in range(batch):
        length8 = jnp.where(row8 == s, lengths[s], length8)
        cum8 = jnp.where(row8 == s, cum[s], cum8)
    last = jnp.sum(jnp.where(pos8 == length8 - 1, cum8, 0.0), axis=-1, keepdims=True)
    bias8 = last - cum8 + new_log
    bias8 = jnp.where(pos8 < length8, bias8, -jnp.inf)
    bias16 = jnp.concatenate([bias8] * groups, axis=0)
    loads[3].wait()
    phase("scores")
    scores = jnp.zeros((n16, cache), F32)
    for s in range(batch):
        scores = jnp.where(row16 == s, nt(q16, keys[s]), scores)
    phase("softmax")
    scale = head ** (-0.5)
    past = jnp.exp(scores * scale + bias16)
    own = jnp.exp(jnp.sum(q16.astype(F32) * new_key, axis=-1, keepdims=True) * scale)
    denominator = jnp.sum(past, axis=-1, keepdims=True) + own
    prob = (past / denominator).astype(BF).astype(F32)
    own_prob = (own / denominator).astype(BF).astype(F32)
    loads[4].wait()
    phase("values")
    mixed = own_prob * new_value
    for s in range(batch):
        mixed = mixed + mm(jnp.where(row16 == s, prob, 0.0).astype(BF), values[s])
    mixed = mixed.astype(BF)
    loads[5].wait()
    phase("outproj")
    heads = jnp.concatenate([mixed[i * batch : (i + 1) * batch] for i in range(groups)], axis=1)
    partial = mm(heads, ow[...]).astype(BF)
    pt[0] = partial

    phase("barrier")
    pl.semaphore_wait(barrier, len(partners))
    for d in (nz // 4, nz - nz // 4):
        pl.semaphore_signal(known, inc=1, device_id=at("z", z, d, nz), device_id_type=MESH)
    phase("tsend")
    for d in (2, 1, 3):
        send(pt.at[0], pt.at[d], tsend, trecv, at("t", t, d, nt_))

    landed(wgu.at[0], lsem.at[6])
    loads[8].wait()
    loads[9].wait()
    there = {"t": partner}
    send(wgu.at[0], wgu.at[1], wsend.at[0], wrecv.at[0], there)
    send(wd.at[0], wd.at[1], wsend.at[1], wrecv.at[1], there)
    send(wsd.at[t], wsd.at[t], wsend.at[2], wrecv.at[2], there)

    phase("route")
    rowm = lax.broadcasted_iota(jnp.int32, (batch, META), 0)
    lane = lax.broadcasted_iota(jnp.int32, (batch, META), 1)
    zero = jnp.zeros((batch, META), F32)
    r0, r1, w0, w1 = zero, zero, zero, zero
    for s in range(batch):
        here = rowm == s
        r0 = jnp.where(here, routes[0, s].astype(F32), r0)
        r1 = jnp.where(here, routes[1, s].astype(F32), r1)
        w0 = jnp.where(here, route_w[0, s], w0)
        w1 = jnp.where(here, route_w[1, s], w1)
    total = w0 + w1
    h0, l0 = hi_lo(w0 / total)
    h1, l1 = hi_lo(w1 / total)
    for i in (10, 11):
        loads[i].wait()

    phase("twait")
    landed(pt.at[1:nt_], trecv)
    residual = tok + pt[0].astype(F32)
    for d in range(1, nt_):
        residual = residual + pt[d].astype(F32)
    phase("ffn")
    ffn = rms(residual, row_of(ffn_gain)).astype(BF).astype(F32)
    gate = jnp.sum(ffn * row_of(mix_w), axis=-1, keepdims=True)
    gate = 1.0 / (1.0 + jnp.exp(-gate))
    hg, lg = hi_lo(jnp.broadcast_to(gate, (batch, META)))
    meta = zero
    for i, v in enumerate((r0, r1, h0, l0, h1, l1, hg, lg)):
        meta = jnp.where(lane == i, v, meta)
    full = jnp.concatenate([ffn, meta], axis=1)
    sel = full[0:rows]
    for k in range(1, nt_):
        sel = jnp.where(t == k, full[k * rows : (k + 1) * rows], sel)
    ob[0] = sel.astype(BF)
    mine8 = residual[:, 0:width]
    for k in range(1, nt_):
        mine8 = jnp.where(t == k, residual[:, k * width : (k + 1) * width], mine8)

    group = lax.div(z, near)

    def give_z(d):
        send(ob.at[0], zb.at[z], zsend, zrecv.at[group], at("z", z, d, nz))

    phase("zsend")
    pltpu.make_async_copy(ob.at[0], zb.at[z], zrecv.at[group]).start()
    by_distance = sorted(range(1, nz), key=lambda d: (-min(d, nz - d), d))
    for d in by_distance:
        if min(d, nz - d) <= nz // 4:
            give_z(d)
    phase("spread2")
    pl.semaphore_wait(known, 2)
    for d in by_distance:
        if min(d, nz - d) > nz // 4:
            give_z(d)

    twin = {"c": 1 - c}
    level = lax.div(t, 2)

    def spot(dx, dq):
        return 2 * idx(x, dx, nx) + (1 - level if dq else level)

    def place_of(dx, dq):
        return {"x": idx(x, dx, nx), "t": idx(t, 2 * dq, nt_)}

    far_first = [(2, 1), (2, 0), (1, 1), (3, 1), (0, 1), (1, 0), (3, 0)]
    me = spot(0, 0)

    def take_z(h):
        phase("zwait#h=%d" % h)
        landed(zb.at[h * near : (h + 1) * near], zrecv.at[h])
        phase("xsend#h=%d" % h)
        g[h, c, me] = zb[h * near : (h + 1) * near].reshape(strip, wide)
        piece = g.at[h, c, me]
        send(piece, piece, ysend, yrecv.at[h], {"t": opp})
        hand_on(h, 0)

    def hand_on(h, dq):
        piece = g.at[h, c, spot(0, dq)]
        for dx in (2, 1, 3):
            send(piece, piece, xsend.at[h], xrecv.at[h, dq], at("x", x, dx, nx))
        send(piece, piece, csend.at[h], crecv.at[h], twin)

    def take_y(h):
        phase("yfwd#h=%d" % h)
        landed(g.at[h, c, spot(0, 1)], yrecv.at[h])
        hand_on(h, 1)

    def take_x(h, dq):
        phase("xwait%d#h=%d" % (dq, h))
        landed(g.at[h, c, 0 : nx - 1], xrecv.at[h, dq])
        for dx in range(1, nx):
            piece = g.at[h, c, spot(dx, dq)]
            send(piece, piece, csend.at[h], crecv.at[h], twin)

    def take_c(h):
        phase("cwait#h=%d" % h)
        landed(g.at[h, 1 - c], crecv.at[h])

    mine = ((z * nx + x) * nc + c).astype(F32)

    def compute(h):
        phase("compute#h=%d" % h)
        every = g[h].reshape(nc * part_rows, wide)
        info = every[:, depth:wide].astype(F32)
        w = jnp.where(info[:, 0:1] == mine, info[:, 2:3] + info[:, 3:4], 0.0)
        w = w + jnp.where(info[:, 1:2] == mine, info[:, 4:5] + info[:, 5:6], 0.0)
        xs = every[:, 0:depth]
        hid = []
        for k in (0, 1):
            pre = mm(xs, wgu[k])
            hid.append((silu(pre[:, 0:hidden]) * pre[:, hidden : 2 * hidden]).astype(BF))
        sh = (silu(nt(xs, sg[...])) * nt(xs, su[...])).astype(BF)
        dense = jnp.concatenate([mm(sh, wsd[k]) for k in range(nt_)], axis=1)
        res = mm(jnp.concatenate(hid, axis=1), wd[...].reshape(2 * hidden, depth))
        value = w * res + (info[:, 6:7] + info[:, 7:8]) * dense
        p3[h] = value.astype(BF).reshape(nc, 2 * nx, strip, depth)
        send_c(h)

    def send_c(h):
        send(p3.at[h, 1 - c], rx1.at[h], c2send.at[h], c2recv.at[h], twin)

    def sum_c(h):
        phase("c2#h=%d" % h)
        landed(rx1.at[h], c2recv.at[h])
        for dx, dq in far_first:
            at_ = spot(dx, dq)
            s1[h, at_] = (p3[h, c, at_].astype(F32) + rx1[h, at_].astype(F32)).astype(BF)
            send(s1.at[h, at_], rx2.at[h, 2 * dx + dq], x2send.at[h], x2recv.at[h], place_of(dx, dq))

    def sum_x(h):
        phase("x2#h=%d" % h)
        acc = p3[h, c, me].astype(F32) + rx1[h, me].astype(F32)
        landed(rx2.at[h, 1 : 2 * nx], x2recv.at[h])
        for i in range(1, 2 * nx):
            acc = acc + rx2[h, i].astype(F32)
        phase("z2send#h=%d" % h)
        base = h * nt_ * near
        for k in range(nt_):
            zs[base + k * near : base + (k + 1) * near] = (
                acc[:, k * width : (k + 1) * width].astype(BF).reshape(near, rows, width)
            )

        def give(i, e):
            there = lax.rem(z + i, near) + h * near
            peer = idx(t, e, nt_)
            piece = zs.at[base + peer * near + there - h * near]

            def remote():
                send(piece, rx3.at[t, z], z2send, z2recv.at[t], {"z": there, "t": peer})

            if i or e:
                remote()
            else:
                pl.when(there != z)(remote)
                pl.when(there == z)(lambda: pltpu.make_async_copy(piece, rx3.at[t, z], z2recv.at[t]).start())

        for i in range(near):
            for e in (2, 1, 3, 0):
                give(i, e)

    for h in range(NG):
        take_z(h)
    for h in range(NG):
        take_y(h)
        take_x(h, 0)
    phase("wwait")
    landed(wgu.at[1], wrecv.at[0])
    landed(wd.at[1], wrecv.at[1])
    landed(wsd.at[partner], wrecv.at[2])
    take_x(0, 1)
    take_x(1, 1)
    take_c(0)
    compute(0)
    take_x(2, 1)
    take_c(1)
    compute(1)
    sum_c(0)
    take_x(3, 1)
    take_c(2)
    compute(2)
    sum_c(1)
    take_c(3)
    compute(3)
    sum_c(2)
    sum_c(3)
    for h in range(NG):
        sum_x(h)
    phase("z2wait")
    for e in range(nt_):
        k = idx(t, e, nt_)
        landed(rx3.at[k], z2recv.at[k])
    phase("result")
    sums = [jnp.sum(rx3[k].astype(F32), axis=0) for k in range(nt_)]
    out[...] = mine8 + jnp.concatenate(sums, axis=0)

    phase("drain")
    landed(pt.at[1:nt_], tsend)
    landed(zb.at[1:nz], zsend)
    landed(wgu.at[0], wsend.at[0])
    landed(wd.at[0], wsend.at[1])
    landed(wsd.at[0], wsend.at[2])
    landed(g.at[0, 0, 0:NG], ysend)
    landed(zs.at[1 : nt_ * nz], z2send)
    for h in range(NG):
        landed(g.at[h, 0, 2 : 2 * nx], xsend.at[h])
        landed(g.at[h, 0], csend.at[h])
        landed(rx1.at[h], c2send.at[h])
        landed(rx2.at[h, 1 : 2 * nx], x2send.at[h])
    phase.close()


def per_device(
    dims, tokens, lengths, cache_keys, cache_values, cache_cum, norm_gain, query_weight, key_weight,
    value_weight, forget_weight, forget_bias, query_gain, key_gain, out_weight, ffn_gain, mix_weight,
    shared_gate, shared_up, shared_down, routes, route_weights, expert_gate, expert_up, expert_down,
):
    nz, nx, nc, ny = dims
    batch, depth = tokens.shape
    cache, head = cache_keys.shape[1], cache_keys.shape[3]
    rows = batch // ny
    width = depth // ny
    strip = nz // NG * rows
    hidden = expert_gate.shape[2]
    nq, nk = query_weight.shape[1], key_weight.shape[1]
    fs = shared_gate.shape[1]
    vm = pl.BlockSpec(memory_space=pltpu.VMEM)
    hb = pl.BlockSpec(memory_space=pltpu.HBM)
    dma = pltpu.SemaphoreType.DMA
    scratch = [
        pltpu.VMEM((batch, depth), BF),
        pltpu.SMEM((batch,), jnp.int32),
        pltpu.VMEM((batch, 1, cache), F32),
        pltpu.VMEM((depth,), BF),
        pltpu.VMEM((1, depth), BF),
        pltpu.VMEM((1, 1), F32),
        pltpu.VMEM((head,), BF),
        pltpu.VMEM((head,), BF),
        pltpu.VMEM((depth,), BF),
        pltpu.VMEM((depth,), BF),
        pltpu.SMEM((routes.shape[1], batch), jnp.int32),
        pltpu.SMEM((routes.shape[1], batch), F32),
        pltpu.VMEM((batch, cache, head), BF),
        pltpu.VMEM((batch, cache, head), BF),
        pltpu.VMEM((depth, nq + 2 * nk), BF),
        pltpu.VMEM((nq, depth), BF),
        pltpu.VMEM((fs, depth), BF),
        pltpu.VMEM((fs, depth), BF),
        pltpu.VMEM((ny, fs, width), BF),
        pltpu.VMEM((2, depth, 2 * hidden), BF),
        pltpu.VMEM((2, hidden, depth), BF),
        pltpu.VMEM((ny, batch, depth), BF),
        pltpu.VMEM((1, rows, depth + META), BF),
        pltpu.VMEM((nz, rows, depth + META), BF),
        pltpu.VMEM((NG, nc, 2 * nx, strip, depth + META), BF),
        pltpu.VMEM((NG, nc, 2 * nx, strip, depth), BF),
        pltpu.VMEM((NG, 2 * nx, strip, depth), BF),
        pltpu.VMEM((NG, 2 * nx, strip, depth), BF),
        pltpu.VMEM((NG, 2 * nx, strip, depth), BF),
        pltpu.VMEM((ny * nz, rows, width), BF),
        pltpu.VMEM((ny, nz, rows, width), BF),
        pltpu.SemaphoreType.REGULAR,
        dma((24,)),
        dma((3,)), dma((3,)),
        dma, dma, dma, dma((NG,)), dma((NG,)), dma((NG, 2)), dma((NG,)), dma((NG,)), dma, dma((NG,)),
        dma((NG,)), dma((NG,)), dma((NG,)), dma((NG,)), dma, dma((ny,)),
    ]
    return pl.pallas_call(
        functools.partial(kernel, dims),
        out_shape=jax.ShapeDtypeStruct((batch, width), F32),
        in_specs=[hb] * 24,
        out_specs=vm,
        scratch_shapes=scratch,
        compiler_params=pltpu.CompilerParams(
            collective_id=0, has_side_effects=True, vmem_limit_bytes=60 * 1024 * 1024
        ),
    )(
        tokens, lengths, cache_cum, norm_gain, forget_weight.T, forget_bias.reshape(1, 1), query_gain, key_gain,
        ffn_gain, mix_weight, routes.T, route_weights.T,
        cache_keys.reshape(batch, cache, head), cache_values.reshape(batch, cache, head),
        query_weight, key_weight, value_weight, out_weight, shared_gate.T, shared_up.T, shared_down,
        expert_gate[0], expert_up[0], expert_down[0],
    ).astype(BF)


def solution(mesh):
    ep, ny = mesh.shape["ep"], mesh.shape["tp"]
    nz, nx, nc = (16, 4, 2) if ep == 128 else (ep // 4, 2, 2)
    finer = Mesh(mesh.devices.reshape(nz, nx, nc, ny), ("z", "x", "c", "t"))
    placed = (
        P(EP, None),
        P(EP),
        P(EP, None, "t", None),
        P(EP, None, "t", None),
        P(EP, "t", None),
        P(),
        P(None, "t"),
        P(None, "t"),
        P(None, "t"),
        P(None, "t"),
        P("t"),
        P(),
        P(),
        P("t", None),
        P(),
        P(),
        P(None, EP),
        P(None, EP),
        P(EP, "t"),
        P(EP, None),
        P(EP, None),
        P(EP, None, "t"),
        P(EP, None, "t"),
        P(EP, "t", None),
    )
    return jax.shard_map(
        functools.partial(per_device, (nz, nx, nc, ny)),
        mesh=finer, in_specs=placed, out_specs=P(EP, "t"), check_vma=False,
    )
```

```python
import functools

import jax
import jax.numpy as jnp
from jax import lax
from jax.experimental import pallas as pl
from jax.experimental.pallas import tpu as pltpu
from jax.sharding import Mesh
from jax.sharding import PartitionSpec as P

MESH = pl.DeviceIdType.MESH
EP = ("z", "x", "c")
EPS = 1e-06
META = 128
BF = jnp.bfloat16
NG = 4
F32 = jnp.float32


def rms(values, gain):
    return values * lax.rsqrt(jnp.mean(values * values, axis=-1, keepdims=True) + EPS) * gain


def row_of(ref):
    return ref[...].astype(F32).reshape(1, -1)


def nt(a, b):
    return lax.dot_general(a, b, (((1,), (1,)), ((), ())), preferred_element_type=F32)


def mm(a, b):
    return jnp.dot(a, b, preferred_element_type=F32)


def silu(v):
    return v / (1.0 + jnp.exp(-v))


class Phases:
    def __init__(self):
        self.open = None

    def __call__(self, name):
        self.close()
        self.open = jax.named_scope(name)
        self.open.__enter__()

    def close(self):
        if self.open is not None:
            self.open.__exit__(None, None, None)
            self.open = None


def hi_lo(v):
    hi = v.astype(BF).astype(F32)
    return hi, (v - hi).astype(BF).astype(F32)


def kernel(
    dims,
    tokens_h, lengths_h, cum_h, norm_gain_h, forget_w_h, forget_b_h, query_gain_h, key_gain_h, ffn_gain_h,
    mix_w_h, routes_h, route_w_h,
    keys_h, values_h, qw_h, kw_h, vw_h, ow_h, sg_h, su_h, sd_h, eg_h, eu_h, ed_h,
    out,
    tokens, lengths, cum, norm_gain, forget_w, forget_b, query_gain, key_gain, ffn_gain, mix_w,
    routes, route_w,
    keys, values, wqkv, ow, sg, su, wsd, wgu, wd,
    pt, ob, za, zb, g, p3, rx1, s1, rx2, zs, rx3,
    known, lsem, wsend, wrecv, tsend, trecv, zsend, zrecv, xsend, xrecv, csend, crecv, ysend, yrecv,
    c2send, c2recv, x2send, x2recv, z2send, z2recv,
):
    nz, nx, nc, nt_ = dims
    phase = Phases()
    z, x, c, t = (lax.axis_index(a) for a in ("z", "x", "c", "t"))
    batch, depth = tokens.shape
    rows = batch // nt_
    head = keys.shape[2]
    cache = keys.shape[1]
    groups = qw_h.shape[1] // head
    width = depth // nt_
    hidden = eg_h.shape[1]
    wide = depth + META
    near = nz // NG
    strip = near * rows
    part_rows = nx * 2 * strip
    def idx(base, step, size):
        return lax.rem(base + (step % size), size)

    def at(axis, base, step, size):
        return {axis: idx(base, step, size)}

    def rcopy(src, dst, ss, rs, dev):
        return pltpu.make_async_remote_copy(
            src_ref=src, dst_ref=dst, send_sem=ss, recv_sem=rs, device_id=dev, device_id_type=MESH
        )

    def send(*args):
        rcopy(*args).start()

    def landed(ref, sem):
        pltpu.make_async_copy(ref, ref, sem).wait()

    phase("entry")
    barrier = pltpu.get_barrier_semaphore()
    partners = (
        [at("t", t, d, nt_) for d in range(1, nt_)]
        + [at("c", c, d, nc) for d in range(1, nc)]
        + [at("x", x, d, nx) for d in range(1, nx)]
    )
    along = [d for d in range(1, nz) if min(d, nz - d) <= nz // 4]

    def tell_z(sem, steps, cores):
        @pl.when(c == 1)
        def _():
            for d in steps:
                for core in cores:
                    pl.semaphore_signal(sem, inc=1, device_id={**at("z", z, d, nz), "c": core}, device_id_type=MESH)

    for dev in partners:
        pl.semaphore_signal(barrier, inc=1, device_id=dev, device_id_type=MESH)
    tell_z(barrier, along, (0, 1))

    def local(i, src, dst):
        return pltpu.make_async_copy(src, dst, lsem.at[i])

    nq, nk = qw_h.shape[1], kw_h.shape[1]
    loads = [
        local(0, qw_h, wqkv.at[:, 0:nq]),
        local(0, kw_h, wqkv.at[:, nq : nq + nk]),
        local(0, vw_h, wqkv.at[:, nq + nk : nq + 2 * nk]),
        local(3, keys_h, keys),
        local(4, values_h, values),
        local(5, ow_h, ow),
        local(6, eg_h, wgu.at[0, :, 0:hidden]),
        local(6, eu_h, wgu.at[0, :, hidden : 2 * hidden]),
        local(8, ed_h, wd.at[0]),
        local(9, sd_h, wsd.at[t]),
        local(10, sg_h, sg),
        local(11, su_h, su),
    ]
    small = [
        local(12 + i, src, dst)
        for i, (src, dst) in enumerate((
            (tokens_h, tokens), (norm_gain_h, norm_gain), (forget_w_h, forget_w), (forget_b_h, forget_b),
            (query_gain_h, query_gain), (key_gain_h, key_gain), (lengths_h, lengths), (cum_h, cum),
            (ffn_gain_h, ffn_gain), (mix_w_h, mix_w), (routes_h, routes), (route_w_h, route_w),
        ))
    ]
    for cp in small + loads:
        cp.start()
    phase("small_wait")
    for cp in small:
        cp.wait()

    opp = idx(t, 2, nt_)
    partner = lax.rem(t + 1 + 2 * lax.rem(t + c, 2), nt_)
    wsd[opp] = jnp.zeros(wsd.shape[1:], BF)
    wsd[idx(partner, 2, nt_)] = jnp.zeros(wsd.shape[1:], BF)

    phase("norm")
    tok = tokens[...].astype(F32)
    normed = rms(tok, row_of(norm_gain)).astype(BF)
    logit = jnp.sum(normed.astype(F32) * forget_w[...].astype(F32), axis=-1, keepdims=True) + forget_b[...]
    new_log = jnp.minimum(logit, 0.0) - jnp.log(1.0 + jnp.exp(-jnp.abs(logit)))
    landed(wqkv, lsem.at[0])
    phase("qkv")
    qkv = mm(normed, wqkv[...])
    qg, kg = row_of(query_gain), row_of(key_gain)
    q16 = jnp.concatenate(
        [rms(qkv[:, i * head : (i + 1) * head], qg).astype(BF) for i in range(groups)], axis=0
    )
    new_key = rms(qkv[:, nq : nq + nk], kg).astype(BF).astype(F32)
    new_value = qkv[:, nq + nk : nq + 2 * nk].astype(BF).astype(F32)
    new_key = jnp.concatenate([new_key] * groups, axis=0)
    new_value = jnp.concatenate([new_value] * groups, axis=0)
    phase("bias")
    n16 = batch * groups
    row16 = lax.rem(lax.broadcasted_iota(jnp.int32, (n16, cache), 0), batch)
    row8 = lax.broadcasted_iota(jnp.int32, (batch, cache), 0)
    pos8 = lax.broadcasted_iota(jnp.int32, (batch, cache), 1)
    length8 = jnp.zeros((batch, cache), jnp.int32)
    cum8 = jnp.zeros((batch, cache), F32)
    for s in range(batch):
        length8 = jnp.where(row8 == s, lengths[s], length8)
        cum8 = jnp.where(row8 == s, cum[s], cum8)
    last = jnp.sum(jnp.where(pos8 == length8 - 1, cum8, 0.0), axis=-1, keepdims=True)
    bias8 = last - cum8 + new_log
    bias8 = jnp.where(pos8 < length8, bias8, -jnp.inf)
    bias16 = jnp.concatenate([bias8] * groups, axis=0)
    loads[3].wait()
    phase("scores")
    scores = jnp.zeros((n16, cache), F32)
    for s in range(batch):
        scores = jnp.where(row16 == s, nt(q16, keys[s]), scores)
    phase("softmax")
    scale = head ** (-0.5)
    past = jnp.exp(scores * scale + bias16)
    own = jnp.exp(jnp.sum(q16.astype(F32) * new_key, axis=-1, keepdims=True) * scale)
    denominator = jnp.sum(past, axis=-1, keepdims=True) + own
    prob = (past / denominator).astype(BF).astype(F32)
    own_prob = (own / denominator).astype(BF).astype(F32)
    loads[4].wait()
    phase("values")
    mixed = own_prob * new_value
    for s in range(batch):
        mixed = mixed + mm(jnp.where(row16 == s, prob, 0.0).astype(BF), values[s])
    mixed = mixed.astype(BF)
    loads[5].wait()
    phase("outproj")
    heads = jnp.concatenate([mixed[i * batch : (i + 1) * batch] for i in range(groups)], axis=1)
    partial = mm(heads, ow[...]).astype(BF)
    pt[0] = partial

    phase("barrier")
    pl.semaphore_wait(barrier, len(partners) + len(along))
    tell_z(known, (nz // 4, nz - nz // 4), (1,))
    phase("tsend")
    for d in (2, 1, 3):
        send(pt.at[0], pt.at[d], tsend, trecv, at("t", t, d, nt_))

    landed(wgu.at[0], lsem.at[6])
    loads[8].wait()
    loads[9].wait()
    there = {"t": partner}
    send(wgu.at[0], wgu.at[1], wsend.at[0], wrecv.at[0], there)
    send(wd.at[0], wd.at[1], wsend.at[1], wrecv.at[1], there)
    send(wsd.at[t], wsd.at[t], wsend.at[2], wrecv.at[2], there)

    phase("route")
    rowm = lax.broadcasted_iota(jnp.int32, (batch, META), 0)
    lane = lax.broadcasted_iota(jnp.int32, (batch, META), 1)
    zero = jnp.zeros((batch, META), F32)
    r0, r1, w0, w1 = zero, zero, zero, zero
    for s in range(batch):
        here = rowm == s
        r0 = jnp.where(here, routes[0, s].astype(F32), r0)
        r1 = jnp.where(here, routes[1, s].astype(F32), r1)
        w0 = jnp.where(here, route_w[0, s], w0)
        w1 = jnp.where(here, route_w[1, s], w1)
    total = w0 + w1
    h0, l0 = hi_lo(w0 / total)
    h1, l1 = hi_lo(w1 / total)
    for i in (10, 11):
        loads[i].wait()

    phase("twait")
    landed(pt.at[1:nt_], trecv)
    residual = tok + pt[0].astype(F32)
    for d in range(1, nt_):
        residual = residual + pt[d].astype(F32)
    phase("ffn")
    ffn = rms(residual, row_of(ffn_gain)).astype(BF).astype(F32)
    gate = jnp.sum(ffn * row_of(mix_w), axis=-1, keepdims=True)
    gate = 1.0 / (1.0 + jnp.exp(-gate))
    hg, lg = hi_lo(jnp.broadcast_to(gate, (batch, META)))
    meta = zero
    for i, v in enumerate((r0, r1, h0, l0, h1, l1, hg, lg)):
        meta = jnp.where(lane == i, v, meta)
    full = jnp.concatenate([ffn, meta], axis=1)
    parity, level = lax.rem(t, 2), lax.div(t, 2)
    for q in (0, 1):
        lo = 2 * q * rows
        ob[q] = jnp.where(parity == 1, full[lo + rows : lo + 2 * rows], full[lo : lo + rows]).astype(BF)
    mine8 = residual[:, 0:width]
    for k in range(1, nt_):
        mine8 = jnp.where(t == k, residual[:, k * width : (k + 1) * width], mine8)

    group = lax.div(z, near)

    def give_z(dev):
        @pl.when(group == 0)
        def _():
            send(ob, za.at[z, c], zsend, zrecv.at[0], dev)

        @pl.when(group != 0)
        def _():
            send(ob.at[level], zb.at[z, c], zsend, zrecv.at[group], dev)

    def keep_z():
        @pl.when(group == 0)
        def _():
            pltpu.make_async_copy(ob, za.at[z, 1], zrecv.at[0]).start()

        @pl.when(group != 0)
        def _():
            pltpu.make_async_copy(ob.at[level], zb.at[z, 1], zrecv.at[group]).start()

    phase("zsend")
    pl.when(c == 0)(lambda: give_z({"c": 1}))
    pl.when(c == 1)(keep_z)
    by_distance = sorted(range(1, nz), key=lambda d: (-min(d, nz - d), d))
    for d in by_distance:
        if d in along:
            give_z({**at("z", z, d, nz), "c": 1})
    phase("spread2")
    pl.semaphore_wait(known, 1 + c)

    @pl.when(c == 1)
    def _():
        pl.semaphore_signal(known, inc=1, device_id={"c": 0}, device_id_type=MESH)

    for d in by_distance:
        if d not in along:
            give_z({**at("z", z, d, nz), "c": 1})

    twin = {"c": 1 - c}

    def spot(dx, dq):
        return 2 * idx(x, dx, nx) + (1 - level if dq else level)

    def place_of(dx, dq):
        return {"x": idx(x, dx, nx), "t": idx(t, 2 * dq, nt_)}

    far_first = [(2, 1), (2, 0), (1, 1), (3, 1), (0, 1), (1, 0), (3, 0)]
    me = spot(0, 0)

    def core1(f):
        return lambda *args: pl.when(c == 1)(lambda: f(*args))

    @core1
    def take_z(h):
        if h == 0:
            landed(za, zrecv.at[0])
            for q in (0, 1):
                for core in (0, 1):
                    g[0, 2 * x + q, core] = za[:, core, q].reshape(strip, wide)
            hand_on(0)
        else:
            landed(zb.at[h * near : (h + 1) * near], zrecv.at[h])
            for core in (0, 1):
                g[h, me, core] = zb[h * near : (h + 1) * near, core].reshape(strip, wide)
            send(g.at[h, me], g.at[h, me], ysend, yrecv.at[h], {"t": opp})

    def hand_on(h):
        for dx in (2, 1, 3):
            for dq in (0, 1):
                piece = g.at[h, spot(0, dq)]
                send(piece, piece, xsend.at[h], xrecv.at[h], at("x", x, dx, nx))
        for dq in (0, 1):
            piece = g.at[h, spot(0, dq)]
            send(piece, piece, csend.at[h], crecv.at[h], {"c": 0})

    @core1
    def take_y(h):
        landed(g.at[h, spot(0, 1)], yrecv.at[h])
        hand_on(h)

    @core1
    def take_x(h):
        landed(g.at[h, 2 : 2 * nx], xrecv.at[h])
        for dx in range(1, nx):
            for dq in (0, 1):
                piece = g.at[h, spot(dx, dq)]
                send(piece, piece, csend.at[h], crecv.at[h], {"c": 0})

    def take_c(h):
        phase("cwait#h=%d" % h)
        pl.when(c == 0)(lambda: landed(g.at[h], crecv.at[h]))

    mine = ((z * nx + x) * nc + c).astype(F32)

    side = depth // 2

    def compute(h):
        phase("compute#h=%d" % h)
        every = g[h].reshape(nc * part_rows, wide)
        info = every[:, depth:wide].astype(F32)
        w = jnp.where(info[:, 0:1] == mine, info[:, 2:3] + info[:, 3:4], 0.0)
        w = w + jnp.where(info[:, 1:2] == mine, info[:, 4:5] + info[:, 5:6], 0.0)
        xs = every[:, 0:depth]
        hid = []
        for k in (0, 1):
            pre = mm(xs, wgu[k])
            hid.append((silu(pre[:, 0:hidden]) * pre[:, hidden : 2 * hidden]).astype(BF))
        sh = (silu(nt(xs, sg[...])) * nt(xs, su[...])).astype(BF)
        dense = jnp.concatenate([mm(sh, wsd[k]) for k in range(nt_)], axis=1)
        res = mm(jnp.concatenate(hid, axis=1), wd[...].reshape(2 * hidden, depth))
        value = w * res + (info[:, 6:7] + info[:, 7:8]) * dense
        value = value.reshape(2 * nx, nc, strip, depth)
        for core in (0, 1):
            for q in (0, 1):
                p3[h, core, q] = value[:, core, :, q * side : (q + 1) * side].reshape(nx, 2 * strip, side).astype(BF)

    def send_c(h):
        send(p3.at[h, 1 - c], rx1.at[h], c2send.at[h], c2recv.at[h], twin)

    def sum_c(h):
        phase("c2#h=%d" % h)
        landed(rx1.at[h], c2recv.at[h])
        for dx, dq in far_first:
            px, q = idx(x, dx, nx), 1 - level if dq else level
            s1[h, q, px] = (p3[h, c, q, px].astype(F32) + rx1[h, q, px].astype(F32)).astype(BF)
            send(s1.at[h, q, px], rx2.at[h, 2 * dx + dq], x2send.at[h], x2recv.at[h], place_of(dx, dq))

    def sum_x(h):
        phase("x2#h=%d" % h)
        acc = p3[h, c, level, x].astype(F32) + rx1[h, level, x].astype(F32)
        landed(rx2.at[h, 1 : 2 * nx], x2recv.at[h])
        for i in range(1, 2 * nx):
            acc = acc + rx2[h, i].astype(F32)
        phase("z2send#h=%d" % h)
        base = h * 2 * near
        for k in (0, 1):
            for q in (0, 1):
                zs[base + k * near : base + (k + 1) * near, q] = (
                    acc[q * strip : (q + 1) * strip, k * width : (k + 1) * width].astype(BF).reshape(near, rows, width)
                )

        def give(i, e):
            there = lax.rem(z + i, near) + h * near
            peer, k = (t + 1 - 2 * parity, 1 - parity) if e else (t, parity)
            piece = zs.at[base + k * near + there - h * near]
            slot = rx3.at[parity, z]

            def remote():
                send(piece, slot, z2send, z2recv.at[parity], {"z": there, "t": peer})

            if i or e:
                remote()
            else:
                pl.when(there != z)(remote)
                pl.when(there == z)(lambda: pltpu.make_async_copy(piece, slot, z2recv.at[parity]).start())

        for i in range(near):
            for e in (1, 0):
                give(i, e)

    for h in range(NG):
        phase("zwait#h=%d" % h)
        take_z(h)
    phase("yfwd#h=1")
    take_y(1)
    phase("xwait#h=0")
    take_x(0)
    phase("yfwd#h=2")
    take_y(2)
    take_y(3)
    phase("wwait")
    landed(wgu.at[1], wrecv.at[0])
    landed(wd.at[1], wrecv.at[1])
    landed(wsd.at[partner], wrecv.at[2])
    take_c(0)
    compute(0)
    send_c(0)
    sum_c(0)
    phase("xwait#h=1")
    take_x(1)
    take_c(1)
    compute(1)
    send_c(1)
    phase("xwait#h=2")
    take_x(2)
    sum_c(1)
    take_c(2)
    compute(2)
    send_c(2)
    sum_x(0)
    phase("xwait#h=3")
    take_x(3)
    sum_c(2)
    take_c(3)
    compute(3)
    send_c(3)
    sum_x(1)
    sum_c(3)
    for h in (2, 3):
        sum_x(h)
    phase("z2wait")
    for p in (0, 1):
        landed(rx3.at[p], z2recv.at[p])
    phase("result")
    sums = [jnp.sum(rx3[p].astype(F32), axis=0) for p in (0, 1)]
    out[...] = mine8 + jnp.concatenate([sums[p][q] for q in (0, 1) for p in (0, 1)], axis=0)

    phase("drain")
    landed(pt.at[1:nt_], tsend)

    @pl.when(group == 0)
    def _():
        pl.when(c == 0)(lambda: landed(zb, zsend))
        pl.when(c == 1)(lambda: landed(zb.at[1:nz], zsend))

    @pl.when(group != 0)
    def _():
        pl.when(c == 0)(lambda: landed(zb.at[:, 0], zsend))
        pl.when(c == 1)(lambda: landed(zb.at[1:nz, 0], zsend))

    landed(wgu.at[0], wsend.at[0])
    landed(wd.at[0], wsend.at[1])
    landed(wsd.at[0], wsend.at[2])

    @pl.when(c == 1)
    def _():
        landed(g.at[0, 1:NG], ysend)
        for h in range(NG):
            landed(g.at[h, 2 : 2 * nx], xsend.at[h])
            landed(g.at[h], csend.at[h])

    landed(zs.at[1 : 2 * nz], z2send)
    for h in range(NG):
        landed(rx1.at[h], c2send.at[h])
        landed(rx2.at[h, 1 : 2 * nx], x2send.at[h])
    phase.close()


def per_device(
    dims, tokens, lengths, cache_keys, cache_values, cache_cum, norm_gain, query_weight, key_weight,
    value_weight, forget_weight, forget_bias, query_gain, key_gain, out_weight, ffn_gain, mix_weight,
    shared_gate, shared_up, shared_down, routes, route_weights, expert_gate, expert_up, expert_down,
):
    nz, nx, nc, ny = dims
    batch, depth = tokens.shape
    cache, head = cache_keys.shape[1], cache_keys.shape[3]
    rows = batch // ny
    width = depth // ny
    strip = nz // NG * rows
    hidden = expert_gate.shape[2]
    nq, nk = query_weight.shape[1], key_weight.shape[1]
    fs = shared_gate.shape[1]
    vm = pl.BlockSpec(memory_space=pltpu.VMEM)
    hb = pl.BlockSpec(memory_space=pltpu.HBM)
    dma = pltpu.SemaphoreType.DMA
    scratch = [
        pltpu.VMEM((batch, depth), BF),
        pltpu.SMEM((batch,), jnp.int32),
        pltpu.VMEM((batch, 1, cache), F32),
        pltpu.VMEM((depth,), BF),
        pltpu.VMEM((1, depth), BF),
        pltpu.VMEM((1, 1), F32),
        pltpu.VMEM((head,), BF),
        pltpu.VMEM((head,), BF),
        pltpu.VMEM((depth,), BF),
        pltpu.VMEM((depth,), BF),
        pltpu.SMEM((routes.shape[1], batch), jnp.int32),
        pltpu.SMEM((routes.shape[1], batch), F32),
        pltpu.VMEM((batch, cache, head), BF),
        pltpu.VMEM((batch, cache, head), BF),
        pltpu.VMEM((depth, nq + 2 * nk), BF),
        pltpu.VMEM((nq, depth), BF),
        pltpu.VMEM((fs, depth), BF),
        pltpu.VMEM((fs, depth), BF),
        pltpu.VMEM((ny, fs, width), BF),
        pltpu.VMEM((2, depth, 2 * hidden), BF),
        pltpu.VMEM((2, hidden, depth), BF),
        pltpu.VMEM((ny, batch, depth), BF),
        pltpu.VMEM((2, rows, depth + META), BF),
        pltpu.VMEM((nz // NG, nc, 2, rows, depth + META), BF),
        pltpu.VMEM((nz, nc, rows, depth + META), BF),
        pltpu.VMEM((NG, 2 * nx, nc, strip, depth + META), BF),
        pltpu.VMEM((NG, nc, 2, nx, 2 * strip, depth // 2), BF),
        pltpu.VMEM((NG, 2, nx, 2 * strip, depth // 2), BF),
        pltpu.VMEM((NG, 2, nx, 2 * strip, depth // 2), BF),
        pltpu.VMEM((NG, 2 * nx, 2 * strip, depth // 2), BF),
        pltpu.VMEM((2 * nz, 2, rows, width), BF),
        pltpu.VMEM((2, nz, 2, rows, width), BF),
        pltpu.SemaphoreType.REGULAR,
        dma((24,)),
        dma((3,)), dma((3,)),
        dma, dma, dma, dma((NG,)), dma((NG,)), dma((NG,)), dma((NG,)), dma((NG,)), dma, dma((NG,)),
        dma((NG,)), dma((NG,)), dma((NG,)), dma((NG,)), dma, dma((2,)),
    ]
    return pl.pallas_call(
        functools.partial(kernel, dims),
        out_shape=jax.ShapeDtypeStruct((batch, width), F32),
        in_specs=[hb] * 24,
        out_specs=vm,
        scratch_shapes=scratch,
        compiler_params=pltpu.CompilerParams(
            collective_id=0, has_side_effects=True, vmem_limit_bytes=60 * 1024 * 1024
        ),
    )(
        tokens, lengths, cache_cum, norm_gain, forget_weight.T, forget_bias.reshape(1, 1), query_gain, key_gain,
        ffn_gain, mix_weight, routes.T, route_weights.T,
        cache_keys.reshape(batch, cache, head), cache_values.reshape(batch, cache, head),
        query_weight, key_weight, value_weight, out_weight, shared_gate.T, shared_up.T, shared_down,
        expert_gate[0], expert_up[0], expert_down[0],
    ).astype(BF)


def solution(mesh):
    ep, ny = mesh.shape["ep"], mesh.shape["tp"]
    nz, nx, nc = (16, 4, 2) if ep == 128 else (ep // 4, 2, 2)
    finer = Mesh(mesh.devices.reshape(nz, nx, nc, ny), ("z", "x", "c", "t"))
    placed = (
        P(EP, None),
        P(EP),
        P(EP, None, "t", None),
        P(EP, None, "t", None),
        P(EP, "t", None),
        P(),
        P(None, "t"),
        P(None, "t"),
        P(None, "t"),
        P(None, "t"),
        P("t"),
        P(),
        P(),
        P("t", None),
        P(),
        P(),
        P(None, EP),
        P(None, EP),
        P(EP, "t"),
        P(EP, None),
        P(EP, None),
        P(EP, None, "t"),
        P(EP, None, "t"),
        P(EP, "t", None),
    )
    return jax.shard_map(
        functools.partial(per_device, (nz, nx, nc, ny)),
        mesh=finer, in_specs=placed, out_specs=P(EP, "t"), check_vma=False,
    )
```

```python
import functools

import jax
import jax.numpy as jnp
from jax import lax
from jax.experimental import pallas as pl
from jax.experimental.pallas import tpu as pltpu
from jax.sharding import Mesh
from jax.sharding import PartitionSpec as P

MESH = pl.DeviceIdType.MESH
EP = ("z", "x", "c")
EPS = 1e-06
META = 128
BF = jnp.bfloat16
NG = 4
F32 = jnp.float32


def rms(values, gain):
    return values * lax.rsqrt(jnp.mean(values * values, axis=-1, keepdims=True) + EPS) * gain


def row_of(ref):
    return ref[...].astype(F32).reshape(1, -1)


def nt(a, b):
    return lax.dot_general(a, b, (((1,), (1,)), ((), ())), preferred_element_type=F32)


def mm(a, b):
    return jnp.dot(a, b, preferred_element_type=F32)


def silu(v):
    return v / (1.0 + jnp.exp(-v))


class Phases:
    def __init__(self):
        self.open = None

    def __call__(self, name):
        self.close()
        self.open = jax.named_scope(name)
        self.open.__enter__()

    def close(self):
        if self.open is not None:
            self.open.__exit__(None, None, None)
            self.open = None


def hi_lo(v):
    hi = v.astype(BF).astype(F32)
    return hi, (v - hi).astype(BF).astype(F32)


def kernel(
    dims,
    tokens_h, lengths_h, cum_h, norm_gain_h, forget_w_h, forget_b_h, query_gain_h, key_gain_h, ffn_gain_h,
    mix_w_h, routes_h, route_w_h,
    keys_h, values_h, qw_h, kw_h, vw_h, ow_h, sg_h, su_h, sd_h, eg_h, eu_h, ed_h,
    out,
    tokens, lengths, cum, norm_gain, forget_w, forget_b, query_gain, key_gain, ffn_gain, mix_w,
    routes, route_w,
    keys, values, wqkv, ow, sg, su, wsd, wgu, wd,
    pt, ob, za, zb, g, p3, rx1, s1, rx2, zs, rx3,
    known, lsem, wsend, wrecv, tsend, trecv, zsend, zrecv, xsend, xrecv, csend, crecv, ysend, yrecv,
    c2send, c2recv, x2send, x2recv, z2send, z2recv,
):
    nz, nx, nc, nt_ = dims
    phase = Phases()
    z, x, c, t = (lax.axis_index(a) for a in ("z", "x", "c", "t"))
    batch, depth = tokens.shape
    rows = batch // nt_
    head = keys.shape[2]
    cache = keys.shape[1]
    groups = qw_h.shape[1] // head
    width = depth // nt_
    hidden = eg_h.shape[1]
    wide = depth + META
    near = nz // NG
    strip = near * rows
    part_rows = nx * 2 * strip
    def idx(base, step, size):
        return lax.rem(base + (step % size), size)

    def at(axis, base, step, size):
        return {axis: idx(base, step, size)}

    def rcopy(src, dst, ss, rs, dev):
        return pltpu.make_async_remote_copy(
            src_ref=src, dst_ref=dst, send_sem=ss, recv_sem=rs, device_id=dev, device_id_type=MESH
        )

    def send(*args):
        rcopy(*args).start()

    def landed(ref, sem):
        pltpu.make_async_copy(ref, ref, sem).wait()

    phase("entry")
    barrier = pltpu.get_barrier_semaphore()
    partners = (
        [at("t", t, d, nt_) for d in range(1, nt_)]
        + [at("c", c, d, nc) for d in range(1, nc)]
        + [at("x", x, d, nx) for d in range(1, nx)]
    )
    along = [d for d in range(1, nz) if min(d, nz - d) <= nz // 4]

    def tell_z(sem, steps, cores):
        @pl.when(c == 1)
        def _():
            for d in steps:
                for core in cores:
                    pl.semaphore_signal(sem, inc=1, device_id={**at("z", z, d, nz), "c": core}, device_id_type=MESH)

    for dev in partners:
        pl.semaphore_signal(barrier, inc=1, device_id=dev, device_id_type=MESH)
    tell_z(barrier, along, (0, 1))

    def local(i, src, dst):
        return pltpu.make_async_copy(src, dst, lsem.at[i])

    nq, nk = qw_h.shape[1], kw_h.shape[1]
    loads = [
        local(0, qw_h, wqkv.at[:, 0:nq]),
        local(0, kw_h, wqkv.at[:, nq : nq + nk]),
        local(0, vw_h, wqkv.at[:, nq + nk : nq + 2 * nk]),
        local(3, keys_h, keys),
        local(4, values_h, values),
        local(5, ow_h, ow),
        local(6, eg_h, wgu.at[0, :, 0:hidden]),
        local(6, eu_h, wgu.at[0, :, hidden : 2 * hidden]),
        local(8, ed_h, wd.at[0]),
        local(9, sd_h, wsd.at[t]),
        local(10, sg_h, sg),
        local(11, su_h, su),
    ]
    small = [
        local(12 + i, src, dst)
        for i, (src, dst) in enumerate((
            (tokens_h, tokens), (norm_gain_h, norm_gain), (forget_w_h, forget_w), (forget_b_h, forget_b),
            (query_gain_h, query_gain), (key_gain_h, key_gain), (lengths_h, lengths), (cum_h, cum),
            (ffn_gain_h, ffn_gain), (mix_w_h, mix_w), (routes_h, routes), (route_w_h, route_w),
        ))
    ]
    for cp in small + loads:
        cp.start()
    phase("small_wait")
    for cp in small:
        cp.wait()

    opp = idx(t, 2, nt_)
    partner = lax.rem(t + 1 + 2 * lax.rem(t + c, 2), nt_)
    wsd[opp] = jnp.zeros(wsd.shape[1:], BF)
    wsd[idx(partner, 2, nt_)] = jnp.zeros(wsd.shape[1:], BF)

    phase("norm")
    tok = tokens[...].astype(F32)
    normed = rms(tok, row_of(norm_gain)).astype(BF)
    logit = jnp.sum(normed.astype(F32) * forget_w[...].astype(F32), axis=-1, keepdims=True) + forget_b[...]
    new_log = jnp.minimum(logit, 0.0) - jnp.log(1.0 + jnp.exp(-jnp.abs(logit)))
    landed(wqkv, lsem.at[0])
    phase("qkv")
    qkv = mm(normed, wqkv[...])
    qg, kg = row_of(query_gain), row_of(key_gain)
    q16 = jnp.concatenate(
        [rms(qkv[:, i * head : (i + 1) * head], qg).astype(BF) for i in range(groups)], axis=0
    )
    new_key = rms(qkv[:, nq : nq + nk], kg).astype(BF).astype(F32)
    new_value = qkv[:, nq + nk : nq + 2 * nk].astype(BF).astype(F32)
    new_key = jnp.concatenate([new_key] * groups, axis=0)
    new_value = jnp.concatenate([new_value] * groups, axis=0)
    phase("bias")
    n16 = batch * groups
    row16 = lax.rem(lax.broadcasted_iota(jnp.int32, (n16, cache), 0), batch)
    row8 = lax.broadcasted_iota(jnp.int32, (batch, cache), 0)
    pos8 = lax.broadcasted_iota(jnp.int32, (batch, cache), 1)
    length8 = jnp.zeros((batch, cache), jnp.int32)
    cum8 = jnp.zeros((batch, cache), F32)
    for s in range(batch):
        length8 = jnp.where(row8 == s, lengths[s], length8)
        cum8 = jnp.where(row8 == s, cum[s], cum8)
    last = jnp.sum(jnp.where(pos8 == length8 - 1, cum8, 0.0), axis=-1, keepdims=True)
    bias8 = last - cum8 + new_log
    bias8 = jnp.where(pos8 < length8, bias8, -jnp.inf)
    bias16 = jnp.concatenate([bias8] * groups, axis=0)
    loads[3].wait()
    phase("scores")
    scores = jnp.zeros((n16, cache), F32)
    for s in range(batch):
        scores = jnp.where(row16 == s, nt(q16, keys[s]), scores)
    phase("softmax")
    scale = head ** (-0.5)
    past = jnp.exp(scores * scale + bias16)
    own = jnp.exp(jnp.sum(q16.astype(F32) * new_key, axis=-1, keepdims=True) * scale)
    denominator = jnp.sum(past, axis=-1, keepdims=True) + own
    prob = (past / denominator).astype(BF).astype(F32)
    own_prob = (own / denominator).astype(BF).astype(F32)
    loads[4].wait()
    phase("values")
    mixed = own_prob * new_value
    for s in range(batch):
        mixed = mixed + mm(jnp.where(row16 == s, prob, 0.0).astype(BF), values[s])
    mixed = mixed.astype(BF)
    loads[5].wait()
    phase("outproj")
    heads = jnp.concatenate([mixed[i * batch : (i + 1) * batch] for i in range(groups)], axis=1)
    partial = mm(heads, ow[...]).astype(BF)
    pt[0] = partial

    phase("barrier")
    pl.semaphore_wait(barrier, len(partners) + len(along))
    tell_z(known, (nz // 4, nz - nz // 4), (1,))
    phase("tsend")
    for d in (2, 1, 3):
        send(pt.at[0], pt.at[d], tsend, trecv, at("t", t, d, nt_))

    landed(wgu.at[0], lsem.at[6])
    loads[8].wait()
    loads[9].wait()
    there = {"t": partner}
    send(wgu.at[0], wgu.at[1], wsend.at[0], wrecv.at[0], there)
    send(wd.at[0], wd.at[1], wsend.at[1], wrecv.at[1], there)
    send(wsd.at[t], wsd.at[t], wsend.at[2], wrecv.at[2], there)

    phase("route")
    rowm = lax.broadcasted_iota(jnp.int32, (batch, META), 0)
    lane = lax.broadcasted_iota(jnp.int32, (batch, META), 1)
    zero = jnp.zeros((batch, META), F32)
    r0, r1, w0, w1 = zero, zero, zero, zero
    for s in range(batch):
        here = rowm == s
        r0 = jnp.where(here, routes[0, s].astype(F32), r0)
        r1 = jnp.where(here, routes[1, s].astype(F32), r1)
        w0 = jnp.where(here, route_w[0, s], w0)
        w1 = jnp.where(here, route_w[1, s], w1)
    total = w0 + w1
    h0, l0 = hi_lo(w0 / total)
    h1, l1 = hi_lo(w1 / total)
    for i in (10, 11):
        loads[i].wait()

    phase("twait")
    landed(pt.at[1:nt_], trecv)
    residual = tok + pt[0].astype(F32)
    for d in range(1, nt_):
        residual = residual + pt[d].astype(F32)
    phase("ffn")
    ffn = rms(residual, row_of(ffn_gain)).astype(BF).astype(F32)
    gate = jnp.sum(ffn * row_of(mix_w), axis=-1, keepdims=True)
    gate = 1.0 / (1.0 + jnp.exp(-gate))
    hg, lg = hi_lo(jnp.broadcast_to(gate, (batch, META)))
    meta = zero
    for i, v in enumerate((r0, r1, h0, l0, h1, l1, hg, lg)):
        meta = jnp.where(lane == i, v, meta)
    full = jnp.concatenate([ffn, meta], axis=1)
    parity, level = lax.rem(t, 2), lax.div(t, 2)
    for q in (0, 1):
        lo = 2 * q * rows
        ob[q] = jnp.where(parity == 1, full[lo + rows : lo + 2 * rows], full[lo : lo + rows]).astype(BF)
    mine8 = residual[:, 0:width]
    for k in range(1, nt_):
        mine8 = jnp.where(t == k, residual[:, k * width : (k + 1) * width], mine8)

    group = lax.div(z, near)

    def give_z(dev):
        @pl.when(group == 0)
        def _():
            send(ob, za.at[z, c], zsend, zrecv.at[0], dev)

        @pl.when(group != 0)
        def _():
            send(ob.at[level], zb.at[z, c], zsend, zrecv.at[group], dev)

    def keep_z():
        @pl.when(group == 0)
        def _():
            pltpu.make_async_copy(ob, za.at[z, 1], zrecv.at[0]).start()

        @pl.when(group != 0)
        def _():
            pltpu.make_async_copy(ob.at[level], zb.at[z, 1], zrecv.at[group]).start()

    phase("zsend")
    pl.when(c == 0)(lambda: give_z({"c": 1}))
    pl.when(c == 1)(keep_z)
    by_distance = sorted(range(1, nz), key=lambda d: (-min(d, nz - d), d))
    for d in by_distance:
        if d in along:
            give_z({**at("z", z, d, nz), "c": 1})
    phase("spread2")
    pl.semaphore_wait(known, 1 + c)

    @pl.when(c == 1)
    def _():
        pl.semaphore_signal(known, inc=1, device_id={"c": 0}, device_id_type=MESH)

    for d in by_distance:
        if d not in along:
            give_z({**at("z", z, d, nz), "c": 1})

    twin = {"c": 1 - c}

    def spot(dx, dq):
        return 2 * idx(x, dx, nx) + (1 - level if dq else level)

    def place_of(dx, dq):
        return {"x": idx(x, dx, nx), "t": idx(t, 2 * dq, nt_)}

    far_first = [(2, 1), (2, 0), (1, 1), (3, 1), (0, 1), (1, 0), (3, 0)]
    me = spot(0, 0)

    def core1(f):
        return lambda *args: pl.when(c == 1)(lambda: f(*args))

    @core1
    def take_z(h):
        if h == 0:
            landed(za, zrecv.at[0])
            for q in (0, 1):
                for core in (0, 1):
                    g[0, 2 * x + q, core] = za[:, core, q].reshape(strip, wide)
            hand_on(0)
        else:
            landed(zb.at[h * near : (h + 1) * near], zrecv.at[h])
            for core in (0, 1):
                g[h, me, core] = zb[h * near : (h + 1) * near, core].reshape(strip, wide)
            send(g.at[h, me], g.at[h, me], ysend, yrecv.at[h], {"t": opp})

    def hand_on(h):
        for dx in (2, 1, 3):
            for dq in (0, 1):
                piece = g.at[h, spot(0, dq)]
                send(piece, piece, xsend, xrecv.at[h, 1 if dx == 2 else 0], at("x", x, dx, nx))
        for dq in (0, 1):
            piece = g.at[h, spot(0, dq)]
            send(piece, piece, csend, crecv.at[h], {"c": 0})

    @core1
    def take_y(h):
        landed(g.at[h, spot(0, 1)], yrecv.at[h])
        hand_on(h)

    @core1
    def take_x(h):
        for i, steps in enumerate(((1, 3), (2,))):
            landed(g.at[h, 0 : 2 * len(steps)], xrecv.at[h, i])
            for dx in steps:
                for dq in (0, 1):
                    piece = g.at[h, spot(dx, dq)]
                    send(piece, piece, csend, crecv.at[h], {"c": 0})

    def take_c(h):
        phase("cwait#h=%d" % h)
        pl.when(c == 0)(lambda: landed(g.at[h], crecv.at[h]))

    mine = ((z * nx + x) * nc + c).astype(F32)

    side = depth // 2

    def compute(h):
        phase("compute#h=%d" % h)
        every = g[h].reshape(nc * part_rows, wide)
        info = every[:, depth:wide].astype(F32)
        w = jnp.where(info[:, 0:1] == mine, info[:, 2:3] + info[:, 3:4], 0.0)
        w = w + jnp.where(info[:, 1:2] == mine, info[:, 4:5] + info[:, 5:6], 0.0)
        xs = every[:, 0:depth]
        hid = []
        for k in (0, 1):
            pre = mm(xs, wgu[k])
            hid.append((silu(pre[:, 0:hidden]) * pre[:, hidden : 2 * hidden]).astype(BF))
        sh = (silu(nt(xs, sg[...])) * nt(xs, su[...])).astype(BF)
        dense = jnp.concatenate([mm(sh, wsd[k]) for k in range(nt_)], axis=1)
        res = mm(jnp.concatenate(hid, axis=1), wd[...].reshape(2 * hidden, depth))
        value = w * res + (info[:, 6:7] + info[:, 7:8]) * dense
        value = value.reshape(2 * nx, nc, strip, depth)
        for core in (0, 1):
            for q in (0, 1):
                p3[h, core, q] = value[:, core, :, q * side : (q + 1) * side].reshape(nx, 2 * strip, side).astype(BF)

    def send_c(h):
        send(p3.at[h, 1 - c], rx1.at[h], c2send, c2recv.at[h], twin)

    def sum_c(h):
        phase("c2#h=%d" % h)
        landed(rx1.at[h], c2recv.at[h])
        for dx, dq in far_first:
            px, q = idx(x, dx, nx), 1 - level if dq else level
            s1[h, q, px] = (p3[h, c, q, px].astype(F32) + rx1[h, q, px].astype(F32)).astype(BF)
            send(s1.at[h, q, px], rx2.at[h, 2 * dx + dq], x2send, x2recv.at[h], place_of(dx, dq))

    def sum_x(h):
        phase("x2#h=%d" % h)
        acc = p3[h, c, level, x].astype(F32) + rx1[h, level, x].astype(F32)
        landed(rx2.at[h, 1 : 2 * nx], x2recv.at[h])
        for i in range(1, 2 * nx):
            acc = acc + rx2[h, i].astype(F32)
        phase("z2send#h=%d" % h)
        base = h * 2 * near
        for k in (0, 1):
            for q in (0, 1):
                zs[base + k * near : base + (k + 1) * near, q] = (
                    acc[q * strip : (q + 1) * strip, k * width : (k + 1) * width].astype(BF).reshape(near, rows, width)
                )

        def give(i, e):
            there = lax.rem(z + i, near) + h * near
            peer, k = (t + 1 - 2 * parity, 1 - parity) if e else (t, parity)
            piece = zs.at[base + k * near + there - h * near]
            slot = rx3.at[parity, z]

            def remote():
                send(piece, slot, z2send, z2recv.at[parity], {"z": there, "t": peer})

            if i or e:
                remote()
            else:
                pl.when(there != z)(remote)
                pl.when(there == z)(lambda: pltpu.make_async_copy(piece, slot, z2recv.at[parity]).start())

        for i in range(near):
            for e in (1, 0):
                give(i, e)

    for h in range(NG):
        phase("zwait#h=%d" % h)
        take_z(h)
    phase("yfwd#h=1")
    take_y(1)
    phase("xwait#h=0")
    take_x(0)
    phase("yfwd#h=2")
    take_y(2)
    phase("wwait")
    landed(wgu.at[1], wrecv.at[0])
    landed(wd.at[1], wrecv.at[1])
    landed(wsd.at[partner], wrecv.at[2])
    take_c(0)
    compute(0)
    send_c(0)
    sum_c(0)
    phase("yfwd#h=3")
    take_y(3)
    phase("xwait#h=1")
    take_x(1)
    take_c(1)
    compute(1)
    send_c(1)
    phase("xwait#h=2")
    take_x(2)
    sum_c(1)
    take_c(2)
    compute(2)
    send_c(2)
    sum_x(0)
    phase("xwait#h=3")
    take_x(3)
    sum_c(2)
    take_c(3)
    compute(3)
    send_c(3)
    sum_x(1)
    sum_c(3)
    for h in (2, 3):
        sum_x(h)
    phase("z2wait")
    for p in (0, 1):
        landed(rx3.at[p], z2recv.at[p])
    phase("result")
    sums = [jnp.sum(rx3[p].astype(F32), axis=0) for p in (0, 1)]
    out[...] = mine8 + jnp.concatenate([sums[p][q] for q in (0, 1) for p in (0, 1)], axis=0)

    phase("drain")
    landed(pt.at[1:nt_], tsend)

    @pl.when(group == 0)
    def _():
        pl.when(c == 0)(lambda: landed(zb, zsend))
        pl.when(c == 1)(lambda: landed(zb.at[1:nz], zsend))

    @pl.when(group != 0)
    def _():
        pl.when(c == 0)(lambda: landed(zb.at[:, 0], zsend))
        pl.when(c == 1)(lambda: landed(zb.at[1:nz, 0], zsend))

    landed(wgu.at[0], wsend.at[0])
    landed(wd.at[0], wsend.at[1])
    landed(wsd.at[0], wsend.at[2])

    @pl.when(c == 1)
    def _():
        landed(g.at[0, 1:NG], ysend)
        landed(g.at[:, 2 : 2 * nx], xsend)
        landed(g, csend)

    landed(zs.at[1 : 2 * nz], z2send)
    landed(rx1, c2send)
    landed(rx2.at[:, 1 : 2 * nx], x2send)
    phase.close()


def per_device(
    dims, tokens, lengths, cache_keys, cache_values, cache_cum, norm_gain, query_weight, key_weight,
    value_weight, forget_weight, forget_bias, query_gain, key_gain, out_weight, ffn_gain, mix_weight,
    shared_gate, shared_up, shared_down, routes, route_weights, expert_gate, expert_up, expert_down,
):
    nz, nx, nc, ny = dims
    batch, depth = tokens.shape
    cache, head = cache_keys.shape[1], cache_keys.shape[3]
    rows = batch // ny
    width = depth // ny
    strip = nz // NG * rows
    hidden = expert_gate.shape[2]
    nq, nk = query_weight.shape[1], key_weight.shape[1]
    fs = shared_gate.shape[1]
    vm = pl.BlockSpec(memory_space=pltpu.VMEM)
    hb = pl.BlockSpec(memory_space=pltpu.HBM)
    dma = pltpu.SemaphoreType.DMA
    scratch = [
        pltpu.VMEM((batch, depth), BF),
        pltpu.SMEM((batch,), jnp.int32),
        pltpu.VMEM((batch, 1, cache), F32),
        pltpu.VMEM((depth,), BF),
        pltpu.VMEM((1, depth), BF),
        pltpu.VMEM((1, 1), F32),
        pltpu.VMEM((head,), BF),
        pltpu.VMEM((head,), BF),
        pltpu.VMEM((depth,), BF),
        pltpu.VMEM((depth,), BF),
        pltpu.SMEM((routes.shape[1], batch), jnp.int32),
        pltpu.SMEM((routes.shape[1], batch), F32),
        pltpu.VMEM((batch, cache, head), BF),
        pltpu.VMEM((batch, cache, head), BF),
        pltpu.VMEM((depth, nq + 2 * nk), BF),
        pltpu.VMEM((nq, depth), BF),
        pltpu.VMEM((fs, depth), BF),
        pltpu.VMEM((fs, depth), BF),
        pltpu.VMEM((ny, fs, width), BF),
        pltpu.VMEM((2, depth, 2 * hidden), BF),
        pltpu.VMEM((2, hidden, depth), BF),
        pltpu.VMEM((ny, batch, depth), BF),
        pltpu.VMEM((2, rows, depth + META), BF),
        pltpu.VMEM((nz // NG, nc, 2, rows, depth + META), BF),
        pltpu.VMEM((nz, nc, rows, depth + META), BF),
        pltpu.VMEM((NG, 2 * nx, nc, strip, depth + META), BF),
        pltpu.VMEM((NG, nc, 2, nx, 2 * strip, depth // 2), BF),
        pltpu.VMEM((NG, 2, nx, 2 * strip, depth // 2), BF),
        pltpu.VMEM((NG, 2, nx, 2 * strip, depth // 2), BF),
        pltpu.VMEM((NG, 2 * nx, 2 * strip, depth // 2), BF),
        pltpu.VMEM((2 * nz, 2, rows, width), BF),
        pltpu.VMEM((2, nz, 2, rows, width), BF),
        pltpu.SemaphoreType.REGULAR,
        dma((24,)),
        dma((3,)), dma((3,)),
        dma, dma, dma, dma((NG,)), dma, dma((NG, 2)), dma, dma((NG,)), dma, dma((NG,)),
        dma, dma((NG,)), dma, dma((NG,)), dma, dma((2,)),
    ]
    return pl.pallas_call(
        functools.partial(kernel, dims),
        out_shape=jax.ShapeDtypeStruct((batch, width), F32),
        in_specs=[hb] * 24,
        out_specs=vm,
        scratch_shapes=scratch,
        compiler_params=pltpu.CompilerParams(
            collective_id=0, has_side_effects=True, vmem_limit_bytes=60 * 1024 * 1024
        ),
    )(
        tokens, lengths, cache_cum, norm_gain, forget_weight.T, forget_bias.reshape(1, 1), query_gain, key_gain,
        ffn_gain, mix_weight, routes.T, route_weights.T,
        cache_keys.reshape(batch, cache, head), cache_values.reshape(batch, cache, head),
        query_weight, key_weight, value_weight, out_weight, shared_gate.T, shared_up.T, shared_down,
        expert_gate[0], expert_up[0], expert_down[0],
    ).astype(BF)


def solution(mesh):
    ep, ny = mesh.shape["ep"], mesh.shape["tp"]
    nz, nx, nc = (16, 4, 2) if ep == 128 else (ep // 4, 2, 2)
    finer = Mesh(mesh.devices.reshape(nz, nx, nc, ny), ("z", "x", "c", "t"))
    placed = (
        P(EP, None),
        P(EP),
        P(EP, None, "t", None),
        P(EP, None, "t", None),
        P(EP, "t", None),
        P(),
        P(None, "t"),
        P(None, "t"),
        P(None, "t"),
        P(None, "t"),
        P("t"),
        P(),
        P(),
        P("t", None),
        P(),
        P(),
        P(None, EP),
        P(None, EP),
        P(EP, "t"),
        P(EP, None),
        P(EP, None),
        P(EP, None, "t"),
        P(EP, None, "t"),
        P(EP, "t", None),
    )
    return jax.shard_map(
        functools.partial(per_device, (nz, nx, nc, ny)),
        mesh=finer, in_specs=placed, out_specs=P(EP, "t"), check_vma=False,
    )
```
